32 devices in a mesh: sp: 8 (over z, y), tp: 4 (over x, core).
Axes of the slice: x: 2, y: 2, z: 4, core: 2. Of those that a mesh axis runs over, the one named last changes fastest.
Arguments:
- tokens: bfloat16 [1024, 2048], P(('sp', 'tp')), may hold values from -70 to 70
- w_query: bfloat16 [2048, 2048], P(None, 'tp'), may hold values from -0.1875 to 0.1875
- w_key: bfloat16 [2048, 1024], P(None, 'tp'), may hold values from -0.1875 to 0.1875
- w_value: bfloat16 [2048, 1024], P(None, 'tp'), may hold values from -0.125 to 0.125
- w_out: bfloat16 [2048, 2048], P('tp'), may hold values from -0.125 to 0.125
- lambda_head: float32 [16], P('tp'), may hold values from 0.3 to 0.8
- sub_gain: float32 [128], replicated, may hold values from 0.1 to 1.9
Outputs:
- mixed_rows: bfloat16 [1024, 2048], P(('sp', 'tp'))
The draws below stay inside these ranges and needn't reach their ends.
All inputs are finite; a program needn't handle non-finite values.
Results may differ from the reference program's by a relative error of at most 0.015.
The reference program's roundings to bfloat16 on the way count: a program that leaves them out, or rounds other values in their place, can miss the bound.
Values may be sent and summed in bfloat16 or wider, within the bound.
A program may use at most 64 MiB of HBM per device.

```python
import math
import jax
import jax.numpy as jnp
from jax import lax

D = 2048
HEADS = 16
KV_HEADS = 8
QK = 64
VD = 128
TOK_DEV = 128
TOKENS = 1024
N_TP = 4


def draw_tokens(key, part):
    subkeys = jax.random.split(key, 2)
    normal_part = jnp.clip(jax.random.normal(subkeys[0], (TOKENS, D), jnp.float32), -5.0, 5.0)
    block_count = TOKENS // TOK_DEV
    offsets = jnp.clip(0.6 * jax.random.normal(subkeys[1], (block_count, D), jnp.float32), -2.0, 2.0)
    drawn = normal_part + jnp.repeat(offsets, TOK_DEV, axis=0)
    return drawn.astype(jnp.bfloat16)


def steps_of(key, dims, cuts, least, top_value):
    loudness = 1.0
    for axis_at, parts in cuts:
        draws = jax.random.uniform(jax.random.fold_in(jax.random.fold_in(key, 6), axis_at), (parts,), jnp.float32, least / len(cuts), top_value / len(cuts))
        loudness = loudness * jnp.repeat(jnp.exp(draws), dims[axis_at] // parts).reshape((-1,) + (1,) * (len(dims) - 1 - axis_at))
    return loudness


def scatter_about(own_key, dims, scale, most, cuts=(), kind=jnp.bfloat16):
    entries = scale * jax.random.normal(own_key, dims, jnp.float32)
    if cuts:
        entries = entries * steps_of(own_key, dims, cuts, -0.22, 0.18)
    return jnp.clip(entries, -most, most).astype(kind)


def setup_inputs(seed: int = 0) -> dict:
    key_of = jax.random.split(jax.random.key(seed), 8)
    return {
        "tokens": draw_tokens(jax.random.fold_in(key_of[7], 71), 0),
        "w_query": scatter_about(key_of[1], (D, HEADS * 2 * QK), (D // 2) ** -0.5, 0.1875, ((1, 4),)),
        "w_key": scatter_about(key_of[2], (D, KV_HEADS * 2 * QK), (D // 2) ** -0.5, 0.1875, ((1, 4),)),
        "w_value": scatter_about(key_of[3], (D, KV_HEADS * VD), D ** -0.5, 0.125, ((1, 4),)),
        "w_out": scatter_about(key_of[4], (HEADS * VD, D), (HEADS * VD) ** -0.5, 0.125, ((0, 4),)),
        "lambda_head": jnp.clip(0.3 + 0.5 * jax.random.uniform(key_of[5], (HEADS,), jnp.float32) ** steps_of(key_of[5], (HEADS,), ((0, 4),), -0.2, 0.2), 0.3, 0.8),
        "sub_gain": jnp.clip(1.0 + 0.18 * jax.random.normal(key_of[6], (VD,), jnp.float32), 0.1, 1.9),
    }


def reference(tokens, w_query, w_key, w_value, w_out, lambda_head, sub_gain):
    queries = jnp.dot(tokens, w_query, preferred_element_type=jnp.float32).astype(jnp.bfloat16)
    queries = queries.reshape(TOKENS, KV_HEADS, 2, 2, QK)
    keys = jnp.dot(tokens, w_key, preferred_element_type=jnp.float32).astype(jnp.bfloat16)
    keys = keys.reshape(TOKENS, KV_HEADS, 2, QK)
    values = jnp.dot(tokens, w_value, preferred_element_type=jnp.float32).astype(jnp.bfloat16)
    values = values.reshape(TOKENS, KV_HEADS, VD)
    block_rows = math.gcd(TOKENS, 512)
    block_count = TOKENS // block_rows
    key_pos = jnp.arange(TOKENS, dtype=jnp.int32)
    lambda_pair = lambda_head.reshape(KV_HEADS, 2)
    score_scale = 1.0 / math.sqrt(QK)

    def one_group(group_index):
        group_queries = lax.dynamic_index_in_dim(queries, group_index, 1, keepdims=False)
        group_keys = lax.dynamic_index_in_dim(keys, group_index, 1, keepdims=False).astype(jnp.float32)
        group_values = lax.dynamic_index_in_dim(values, group_index, 1, keepdims=False).astype(jnp.float32)
        group_lambda = lax.dynamic_index_in_dim(lambda_pair, group_index, 0, keepdims=False)

        def one_block(block_index):
            first_row = (block_index * block_rows).astype(jnp.int32)
            block_queries = lax.dynamic_slice_in_dim(group_queries, first_row, block_rows, 0).astype(jnp.float32)
            scores = jnp.einsum('tgmd,smd->gmts', block_queries, group_keys) * score_scale
            query_pos = first_row + jnp.arange(block_rows, dtype=jnp.int32)
            allowed = key_pos[None, :] <= query_pos[:, None]
            scores = jnp.where(allowed, scores, -jnp.inf)
            row_peak = lax.optimization_barrier(jnp.max(scores, axis=-1, keepdims=True))
            exponent = jnp.exp(scores - row_peak)
            row_total = lax.optimization_barrier(jnp.sum(exponent, axis=-1))
            weights = lax.optimization_barrier(exponent.astype(jnp.bfloat16)).astype(jnp.float32)
            summed = jnp.einsum('gmts,se->gmte', weights, group_values)
            normalized = summed / row_total[..., None]
            mixed_out = normalized[:, 0] - group_lambda[:, None, None] * normalized[:, 1]
            inverse_rms = lax.rsqrt(lax.optimization_barrier(jnp.mean(mixed_out * mixed_out, axis=-1, keepdims=True)) + 1e-06)
            return (mixed_out * inverse_rms * sub_gain).astype(jnp.bfloat16)
        blocks = lax.map(one_block, jnp.arange(block_count, dtype=jnp.int32))
        return jnp.transpose(blocks, (0, 2, 1, 3)).reshape(TOKENS, 2, VD)
    grouped = lax.map(one_group, jnp.arange(KV_HEADS, dtype=jnp.int32))
    heads = jnp.transpose(grouped, (1, 0, 2, 3)).reshape(TOKENS, HEADS * VD)
    group_width = HEADS * VD // N_TP

    def add_group(group_index, running):
        begin_col = (group_index * group_width).astype(jnp.int32)
        head_part = lax.dynamic_slice_in_dim(heads, begin_col, group_width, 1)
        weight_part = lax.dynamic_slice_in_dim(w_out, begin_col, group_width, 0)
        partial_out = jnp.dot(head_part, weight_part, preferred_element_type=jnp.float32).astype(jnp.bfloat16)
        return running + lax.optimization_barrier(partial_out).astype(jnp.float32)
    summed_out = lax.fori_loop(0, N_TP, add_group, jnp.zeros((TOKENS, D), jnp.float32))
    return summed_out.astype(jnp.bfloat16)
```

```python
import functools
import math

import jax
import jax.numpy as jnp
from jax import lax
from jax.experimental import pallas as pl
from jax.experimental.pallas import tpu as pltpu
from jax.sharding import PartitionSpec as P

QK = 64
VD = 128
MESH = pl.DeviceIdType.MESH
F32 = jnp.float32
BF16 = jnp.bfloat16


def kernel(
    sp_size,
    tp_size,
    tok_hbm,
    wq_hbm,
    wk_hbm,
    wv_hbm,
    wo_hbm,
    lam_ref,
    gain_ref,
    out_ref,
    tok,
    wq,
    wk,
    wv,
    wo,
    kv,
    q_t,
    acc,
    peak,
    total,
    heads,
    part,
    from_sib,
    pair_out,
    pair_in,
    load_sem,
    tok_send,
    tok_fwd,
    tok_recv,
    kv_next,
    kv_side,
    kv_recv,
    sib_send,
    sib_recv,
    pair_send,
    pair_recv,
):
    pairs = tp_size // 2
    rows = tok.shape[2]
    depth = tok.shape[3]
    count = pairs * 2 * rows
    key_cols = wk.shape[1]
    groups = key_cols // (2 * QK)
    subs = 2 * groups
    chunks, width = part.shape[0], part.shape[4]

    sp = lax.axis_index("sp")
    tp = lax.axis_index("tp")
    pair = tp // 2
    core = lax.rem(tp, 2)
    sibling = tp + 1 - 2 * core
    inner = lax.rem(sp, 2)
    outer = sp // 2
    side = sp + 1 - 2 * inner
    has_next = sp + 2 < sp_size
    has_prev = sp >= 2

    def far(step):
        return lax.rem(pair + step, pairs)

    def near(step):
        return lax.rem(pair + pairs - step, pairs)

    load_tok = pltpu.make_async_copy(tok_hbm, tok.at[pair, core], load_sem.at[0])
    load_wk = pltpu.make_async_copy(wk_hbm, wk, load_sem.at[1])
    load_wv = pltpu.make_async_copy(wv_hbm, wv, load_sem.at[2])
    load_wq = pltpu.make_async_copy(wq_hbm, wq, load_sem.at[3])
    load_wo = pltpu.make_async_copy(wo_hbm, wo, load_sem.at[4])
    for load in (load_tok, load_wk, load_wv, load_wq, load_wo):
        load.start()

    barrier = pltpu.get_barrier_semaphore()
    pl.semaphore_signal(barrier, inc=1, device_id={"tp": sibling}, device_id_type=MESH)
    for step in range(1, pairs):
        pl.semaphore_signal(
            barrier, inc=1, device_id={"tp": far(step) * 2 + core}, device_id_type=MESH
        )
    pl.semaphore_signal(barrier, inc=1, device_id={"sp": side}, device_id_type=MESH)

    @pl.when(has_next)
    def _():
        pl.semaphore_signal(barrier, inc=1, device_id={"sp": sp + 2}, device_id_type=MESH)

    @pl.when(has_prev)
    def _():
        pl.semaphore_signal(barrier, inc=1, device_id={"sp": sp - 2}, device_id_type=MESH)

    pl.semaphore_wait(barrier, 1 + pairs + has_next.astype(jnp.int32) + has_prev.astype(jnp.int32))

    def tok_copy(slot_pair, slot_core, sem, device):
        slot = tok.at[slot_pair, slot_core]
        return pltpu.make_async_remote_copy(
            src_ref=slot,
            dst_ref=slot,
            send_sem=sem,
            recv_sem=tok_recv.at[slot_pair, slot_core],
            device_id={"tp": device},
            device_id_type=MESH,
        )

    load_tok.wait()
    far_sends = [
        tok_copy(pair, core, tok_send.at[step], far(step) * 2 + core) for step in range(1, pairs)
    ]
    own_send = tok_copy(pair, core, tok_send.at[0], sibling)
    for copy in far_sends:
        copy.start()
    own_send.start()

    def kv_copy(block, chunk, sub, sems, device):
        slot = kv.at[block, chunk, sub]
        return pltpu.make_async_remote_copy(
            src_ref=slot,
            dst_ref=slot,
            send_sem=sems.at[block, chunk, sub],
            recv_sem=kv_recv.at[block, chunk, sub],
            device_id={"sp": device},
            device_id_type=MESH,
        )

    def pass_on(block, chunk, sub):
        @pl.when(has_next)
        def _():
            kv_copy(block, chunk, sub, kv_next, sp + 2).start()

        @pl.when(block < side)
        def _():
            kv_copy(block, chunk, sub, kv_side, side).start()

    def sent(block, chunk, sub):
        @pl.when(has_next)
        def _():
            kv_copy(block, chunk, sub, kv_next, sp + 2).wait_send()

        @pl.when(block < side)
        def _():
            kv_copy(block, chunk, sub, kv_side, side).wait_send()

    def arrived(block, chunk, sub):
        kv_copy(block, chunk, sub, kv_side, side).wait_recv()

    def relay(block, step):
        for sub in range(subs):
            arrived(block, near(step), sub)
            pass_on(block, near(step), sub)

    def project(chunk):
        x = tok[chunk].reshape(2 * rows, depth)
        for first, weight in ((0, wk), (groups, wv)):
            made = jnp.dot(x, weight[...], preferred_element_type=F32).astype(BF16)
            for g in range(groups):
                kv[sp, chunk, first + g] = made[:, g * VD : (g + 1) * VD]
                pass_on(sp, chunk, first + g)

    gain_t = jnp.broadcast_to(gain_ref[...], (count, VD)).T

    tok_copy(pair, 1 - core, tok_send.at[0], sibling).wait_recv()
    load_wk.wait()
    load_wv.wait()
    project(pair)
    fwds = []
    for step in range(1, pairs):
        source = near(step)
        tok_copy(source, core, tok_send.at[0], sibling).wait_recv()
        fwd = tok_copy(source, core, tok_fwd.at[step], sibling)
        fwd.start()
        fwds.append(fwd)

    @pl.when(has_prev)
    def _():
        relay(sp - 2, 0)

    for step in range(1, pairs):
        source = near(step)
        tok_copy(source, 1 - core, tok_send.at[0], sibling).wait_recv()
        project(source)

    load_wq.wait()
    queries = jnp.dot(tok[...].reshape(count, depth), wq[...], preferred_element_type=F32)
    queries = queries.astype(BF16).astype(F32) * (1.0 / math.sqrt(QK))
    map_of = lax.broadcasted_iota(jnp.int32, (2 * QK, count), 0) // QK
    for g in range(groups):
        for k in range(2):
            at = (g * 2 + k) * 2 * QK
            turned = queries[:, at : at + 2 * QK].T
            for m in range(2):
                q_t[g, :, pl.ds((k * 2 + m) * count, count)] = jnp.where(
                    map_of == m, turned, 0.0
                ).astype(BF16)

    wide = 4 * count

    def absorb(block, first):
        for g in range(groups):
            keys = kv[block, :, g].reshape(count, 2 * QK)
            values = kv[block, :, groups + g].reshape(count, VD)
            scores = jnp.dot(keys, q_t[g], preferred_element_type=F32)
            if first:
                key_at = lax.broadcasted_iota(jnp.int32, (count, wide), 0)
                query_at = lax.rem(lax.broadcasted_iota(jnp.int32, (count, wide), 1), count)
                scores = jnp.where(key_at <= query_at, scores, -jnp.inf)
            top = jnp.max(scores, axis=0, keepdims=True)
            if not first:
                old = peak[g]
                top = jnp.maximum(top, old)
                fade = jnp.exp(old - top)
            expo = jnp.exp(scores - top)
            amount = jnp.sum(expo, axis=0, keepdims=True)
            summed = lax.dot_general(
                values, expo.astype(BF16), (((0,), (0,)), ((), ())), preferred_element_type=F32
            )
            if not first:
                amount = amount + total[g] * fade
                summed = summed + acc[g] * fade
            peak[g] = top
            total[g] = amount
            acc[g] = summed

    absorb(sp, True)

    def turn(d, carried):
        block = sp - 2 * d

        @pl.when(d < outer)
        def _():
            relay(block - 2, 0)

        for step in range(1, pairs):
            relay(block, step)
        absorb(block, False)
        return carried

    lax.fori_loop(1, outer + 1, turn, 0)

    def beside(d, carried):
        block = side - 2 * d
        for step in range(pairs):
            for sub in range(subs):
                arrived(block, near(step), sub)
        absorb(block, False)
        return carried

    lax.fori_loop(1 - inner, outer + 1, beside, 0)

    for g in range(groups):
        for k in range(2):
            left = pl.ds((k * 2) * count, count)
            right = pl.ds((k * 2 + 1) * count, count)
            mixed = acc[g, :, left] / total[g, :, left] - lam_ref[g * 2 + k] * (
                acc[g, :, right] / total[g, :, right]
            )
            power = jnp.mean(mixed * mixed, axis=0, keepdims=True)
            head = mixed * lax.rsqrt(power + 1e-6) * gain_t
            heads[:, (g * 2 + k) * VD : (g * 2 + k + 1) * VD] = head.T.astype(BF16)

    load_wo.wait()

    def sib_copy(j):
        return pltpu.make_async_remote_copy(
            src_ref=part.at[j, 1 - core],
            dst_ref=from_sib.at[j],
            send_sem=sib_send.at[j],
            recv_sem=sib_recv.at[j],
            device_id={"tp": sibling},
            device_id_type=MESH,
        )

    def pair_copy(j, step):
        return pltpu.make_async_remote_copy(
            src_ref=pair_out.at[j, step],
            dst_ref=pair_in.at[j, step],
            send_sem=pair_send.at[j, step],
            recv_sem=pair_recv.at[j, step],
            device_id={"tp": far(step) * 2 + core},
            device_id_type=MESH,
        )

    for j in range(chunks):
        partial = jnp.dot(
            heads[...], wo[:, j * width : (j + 1) * width], preferred_element_type=F32
        ).astype(BF16)
        for p in range(pairs):
            for c in range(2):
                at = (p * 2 + c) * rows
                part[j, c, p] = partial[at : at + rows]
        sib_copy(j).start()
    for j in range(chunks):
        sib_copy(j).wait_recv()
        for step in range(1, pairs):
            goal = far(step)
            pair_out[j, step] = (
                part[j, core, goal].astype(F32) + from_sib[j, goal].astype(F32)
            ).astype(BF16)
            pair_copy(j, step).start()
    for j in range(chunks):
        result = part[j, core, pair].astype(F32) + from_sib[j, pair].astype(F32)
        for step in range(1, pairs):
            pair_copy(j, step).wait_recv()
            result = result + pair_in[j, step].astype(F32)
        out_ref[:, j * width : (j + 1) * width] = result.astype(BF16)

    own_send.wait_send()
    for copy in far_sends + fwds:
        copy.wait_send()

    def drain(d, carried):
        for step in range(pairs):
            for sub in range(subs):
                sent(sp - 2 * d, near(step), sub)
        return carried

    lax.fori_loop(0, outer + 1, drain, 0)
    for j in range(chunks):
        sib_copy(j).wait_send()
        for step in range(1, pairs):
            pair_copy(j, step).wait_send()


def body(sp_size, tp_size, tokens, w_query, w_key, w_value, w_out, lambda_head, sub_gain):
    rows, depth = tokens.shape
    pairs = tp_size // 2
    count = rows * tp_size
    key_cols = w_key.shape[1]
    groups = key_cols // (2 * QK)
    subs = 2 * groups
    out_cols = w_out.shape[1]
    chunks = math.gcd(out_cols // 128, 4)
    width = out_cols // chunks
    anywhere = pl.BlockSpec(memory_space=pl.ANY)
    dma = pltpu.SemaphoreType.DMA
    return pl.pallas_call(
        functools.partial(kernel, sp_size, tp_size),
        out_shape=pltpu.VMEM((rows, out_cols), BF16),
        in_specs=[anywhere] * 5
        + [pl.BlockSpec(memory_space=pltpu.SMEM), pl.BlockSpec(memory_space=pltpu.VMEM)],
        out_specs=pl.BlockSpec(memory_space=pltpu.VMEM),
        scratch_shapes=[
            pltpu.VMEM((pairs, 2, rows, depth), BF16),
            pltpu.VMEM(w_query.shape, BF16),
            pltpu.VMEM(w_key.shape, BF16),
            pltpu.VMEM(w_value.shape, BF16),
            pltpu.VMEM(w_out.shape, BF16),
            pltpu.VMEM((sp_size, pairs, subs, 2 * rows, VD), BF16),
            pltpu.VMEM((groups, 2 * QK, 4 * count), BF16),
            pltpu.VMEM((groups, VD, 4 * count), F32),
            pltpu.VMEM((groups, 1, 4 * count), F32),
            pltpu.VMEM((groups, 1, 4 * count), F32),
            pltpu.VMEM((count, groups * 2 * VD), BF16),
            pltpu.VMEM((chunks, 2, pairs, rows, width), BF16),
            pltpu.VMEM((chunks, pairs, rows, width), BF16),
            pltpu.VMEM((chunks, pairs, rows, width), BF16),
            pltpu.VMEM((chunks, pairs, rows, width), BF16),
            dma((5,)),
            dma((pairs,)),
            dma((pairs,)),
            dma((pairs, 2)),
            dma((sp_size, pairs, subs)),
            dma((sp_size, pairs, subs)),
            dma((sp_size, pairs, subs)),
            dma((chunks,)),
            dma((chunks,)),
            dma((chunks, pairs)),
            dma((chunks, pairs)),
        ],
        compiler_params=pltpu.CompilerParams(
            collective_id=0, has_side_effects=True, vmem_limit_bytes=60 * 1024 * 1024
        ),
    )(tokens, w_query, w_key, w_value, w_out, lambda_head, sub_gain.reshape(1, VD))


def solution(mesh):
    return jax.shard_map(
        functools.partial(body, mesh.shape["sp"], mesh.shape["tp"]),
        mesh=mesh,
        in_specs=(
            P(("sp", "tp"), None),
            P(None, "tp"),
            P(None, "tp"),
            P(None, "tp"),
            P("tp", None),
            P("tp"),
            P(),
        ),
        out_specs=P(("sp", "tp"), None),
        check_vma=False,
    )
```

```python
import functools
import math

import jax
import jax.numpy as jnp
from jax import lax
from jax.experimental import pallas as pl
from jax.experimental.pallas import tpu as pltpu
from jax.sharding import PartitionSpec as P

QK = 64
VD = 128
MESH = pl.DeviceIdType.MESH
F32 = jnp.float32
BF16 = jnp.bfloat16


def kernel(
    sp_size,
    tp_size,
    tok_hbm,
    wq_hbm,
    wk_hbm,
    wv_hbm,
    wo_hbm,
    lam_ref,
    gain_ref,
    out_ref,
    tok,
    wq,
    wkv,
    wo,
    kv,
    q_t,
    acc,
    peak,
    total,
    heads,
    part,
    from_sib,
    pair_out,
    pair_in,
    load_sem,
    tok_send,
    tok_recv,
    kv_next,
    kv_side,
    kv_recv,
    out_send,
    sib_recv,
    pair_recv,
):
    pairs = tp_size // 2
    half = tok.shape[3]
    rows = 2 * half
    depth = tok.shape[4]
    count = pairs * 2 * rows
    key_cols = wkv.shape[2]
    groups = key_cols // (2 * QK)
    chunks, width = part.shape[0], part.shape[4]

    sp = lax.axis_index("sp")
    tp = lax.axis_index("tp")
    pair = tp // 2
    core = lax.rem(tp, 2)
    sibling = tp + 1 - 2 * core
    inner = lax.rem(sp, 2)
    outer = sp // 2
    side = sp + 1 - 2 * inner
    has_next = sp + 2 < sp_size
    has_prev = sp >= 2

    def far(step):
        return lax.rem(pair + step, pairs)

    def near(step):
        return lax.rem(pair + pairs - step, pairs)

    for h in range(2):
        pltpu.make_async_copy(
            tok_hbm.at[pl.ds(h * half, half)], tok.at[pair, core, h], load_sem.at[0]
        ).start()
    load_tok = pltpu.make_async_copy(tok.at[pair, core], tok.at[pair, core], load_sem.at[0])
    pltpu.make_async_copy(wk_hbm, wkv.at[0], load_sem.at[1]).start()
    pltpu.make_async_copy(wv_hbm, wkv.at[1], load_sem.at[1]).start()
    load_kv = pltpu.make_async_copy(wkv, wkv, load_sem.at[1])
    load_wq = pltpu.make_async_copy(wq_hbm, wq, load_sem.at[2])
    load_wo = pltpu.make_async_copy(wo_hbm, wo, load_sem.at[3])
    load_wq.start()
    load_wo.start()

    barrier = pltpu.get_barrier_semaphore()
    pl.semaphore_signal(barrier, inc=1, device_id={"tp": sibling}, device_id_type=MESH)
    for step in range(1, pairs):
        pl.semaphore_signal(
            barrier, inc=1, device_id={"tp": far(step) * 2 + core}, device_id_type=MESH
        )
    pl.semaphore_signal(barrier, inc=1, device_id={"sp": side}, device_id_type=MESH)

    @pl.when(has_next)
    def _():
        pl.semaphore_signal(barrier, inc=1, device_id={"sp": sp + 2}, device_id_type=MESH)

    @pl.when(has_prev)
    def _():
        pl.semaphore_signal(barrier, inc=1, device_id={"sp": sp - 2}, device_id_type=MESH)

    pl.semaphore_wait(barrier, 1 + pairs + has_next.astype(jnp.int32) + has_prev.astype(jnp.int32))

    def tok_copy(slot, sem, recv, device):
        return pltpu.make_async_remote_copy(
            src_ref=slot,
            dst_ref=slot,
            send_sem=sem,
            recv_sem=recv,
            device_id={"tp": device},
            device_id_type=MESH,
        )

    def far_recv(step, role, h):
        return tok_recv.at[1 + ((step - 1) * 2 + role) * 2 + h]

    load_tok.wait()
    for h in range(2):
        for step in range(1, pairs):
            slot = tok.at[pair, core, h]
            goal = far(step) * 2 + core
            tok_copy(slot, tok_send.at[0], far_recv(step, 0, h), goal).start()
        if h == 0:
            tok_copy(tok.at[pair, core], tok_send.at[0], tok_recv.at[0], sibling).start()

    other = 1 - core
    cores = (core, other)

    def kv_at(block, step, role, h):
        chunk = near(step) if step else pair
        if step == 0:
            return kv.at[block, chunk, cores[role]], kv_recv.at[block, role]
        return (
            kv.at[block, chunk, cores[role], h],
            kv_recv.at[block, 2 + ((step - 1) * 2 + role) * 2 + h],
        )

    def kv_copy(slot, sem, recv, device):
        return pltpu.make_async_remote_copy(
            src_ref=slot,
            dst_ref=slot,
            send_sem=sem,
            recv_sem=recv,
            device_id={"sp": device},
            device_id_type=MESH,
        )

    def pass_on(d, step, role, h):
        block = sp - 2 * d
        slot, recv = kv_at(block, step, role, h)

        @pl.when(has_next)
        def _():
            kv_copy(slot, kv_next.at[d], recv, sp + 2).start()

        @pl.when(block < side)
        def _():
            kv_copy(slot, kv_side.at[d], recv, side).start()

    def sent(d):
        block = sp - 2 * d
        whole = kv.at[block]

        @pl.when(has_next)
        def _():
            kv_copy(whole, kv_next.at[d], kv_recv.at[0, 0], sp + 2).wait_send()

        @pl.when(block < side)
        def _():
            kv_copy(whole, kv_side.at[d], kv_recv.at[0, 0], side).wait_send()

    def arrived(block, step, role, h):
        slot, recv = kv_at(block, step, role, h)
        kv_copy(slot, kv_side.at[0], recv, side).wait_recv()

    def relay(d, step, role, h):
        arrived(sp - 2 * d, step, role, h)
        pass_on(d, step, role, h)

    def relay_near(d, role):
        @pl.when(d <= outer)
        def _():
            relay(d, 0, role, 0)

    def relay_far(d, role, h):
        @pl.when(d <= outer)
        def _():
            for step in range(1, pairs):
                relay(d, step, role, h)

    gain_t = jnp.broadcast_to(gain_ref[...], (count, VD)).T
    def project_near(role):
        c = cores[role]
        x = tok[pair, c].reshape(rows, depth)
        for s in range(2):
            made = jnp.dot(x, wkv[s], preferred_element_type=F32).astype(BF16)
            for h in range(2):
                kv[sp, pair, c, h, s] = made[h * half : (h + 1) * half]
        pass_on(0, 0, role, 0)

    def project_far(role, h):
        c = cores[role]
        for step in range(1, pairs):
            source = near(step)
            for s in range(2):
                kv[sp, source, c, h, s] = jnp.dot(
                    tok[source, c, h], wkv[s], preferred_element_type=F32
                ).astype(BF16)
            pass_on(0, step, role, h)

    def receive(role, h):
        for step in range(1, pairs):
            slot = tok.at[near(step), (core, other)[role], h]
            tok_copy(slot, tok_send.at[0], far_recv(step, role, h), sibling).wait_recv()

    def forward(h):
        receive(0, h)
        for step in range(1, pairs):
            slot = tok.at[near(step), core, h]
            tok_copy(slot, tok_send.at[1], far_recv(step, 1, h), sibling).start()

    load_kv.wait()
    project_near(0)
    tok_copy(tok.at[pair, other], tok_send.at[0], tok_recv.at[0], sibling).wait_recv()
    project_near(1)

    forward(0)
    project_far(0, 0)
    relay_near(1, 0)
    receive(1, 0)
    project_far(1, 0)
    relay_near(1, 1)
    forward(1)
    project_far(0, 1)
    receive(1, 1)
    project_far(1, 1)
    relay_near(2, 0)

    load_wq.wait()
    queries = jnp.dot(tok[...].reshape(count, depth), wq[...], preferred_element_type=F32)
    queries = queries.astype(BF16).astype(F32) * (1.0 / math.sqrt(QK))
    map_of = lax.broadcasted_iota(jnp.int32, (2 * QK, count), 0) // QK
    for g in range(groups):
        for k in range(2):
            at = (g * 2 + k) * 2 * QK
            turned = queries[:, at : at + 2 * QK].T
            for m in range(2):
                q_t[g, :, pl.ds((k * 2 + m) * count, count)] = jnp.where(
                    map_of == m, turned, 0.0
                ).astype(BF16)

    relay_far(1, 0, 0)
    relay_near(2, 1)
    relay_far(1, 1, 0)
    wide = 4 * count

    def absorb(block, first):
        for g in range(groups):
            lanes = slice(g * VD, (g + 1) * VD)
            keys = kv[block, :, :, :, 0, :, lanes].reshape(count, 2 * QK)
            values = kv[block, :, :, :, 1, :, lanes].reshape(count, VD)
            scores = jnp.dot(keys, q_t[g], preferred_element_type=F32)
            if first:
                key_at = lax.broadcasted_iota(jnp.int32, (count, wide), 0)
                query_at = lax.rem(lax.broadcasted_iota(jnp.int32, (count, wide), 1), count)
                scores = jnp.where(key_at <= query_at, scores, -jnp.inf)
            top = jnp.max(scores, axis=0, keepdims=True)
            if not first:
                old = peak[g]
                top = jnp.maximum(top, old)
                fade = jnp.exp(old - top)
            expo = jnp.exp(scores - top)
            amount = jnp.sum(expo, axis=0, keepdims=True)
            summed = lax.dot_general(
                values, expo.astype(BF16), (((0,), (0,)), ((), ())), preferred_element_type=F32
            )
            if not first:
                amount = amount + total[g] * fade
                summed = summed + acc[g] * fade
            peak[g] = top
            total[g] = amount
            acc[g] = summed

    absorb(sp, True)

    def turn(d, carried):
        for role in range(2):
            relay_near(d + 2, role)
        for role in range(2):
            relay_far(d + 1, role, 0)
        for role in range(2):
            relay_far(d, role, 1)
        absorb(sp - 2 * d, False)
        return carried

    lax.fori_loop(1, outer + 1, turn, 0)

    def beside(d, carried):
        block = side - 2 * d
        for role in range(2):
            arrived(block, 0, role, 0)
        for step in range(1, pairs):
            for h in range(2):
                for role in range(2):
                    arrived(block, step, role, h)
        absorb(block, False)
        return carried

    lax.fori_loop(1 - inner, outer + 1, beside, 0)

    for g in range(groups):
        for k in range(2):
            left = pl.ds((k * 2) * count, count)
            right = pl.ds((k * 2 + 1) * count, count)
            mixed = acc[g, :, left] / total[g, :, left] - lam_ref[g * 2 + k] * (
                acc[g, :, right] / total[g, :, right]
            )
            power = jnp.mean(mixed * mixed, axis=0, keepdims=True)
            head = mixed * lax.rsqrt(power + 1e-6) * gain_t
            heads[:, (g * 2 + k) * VD : (g * 2 + k + 1) * VD] = head.T.astype(BF16)

    load_wo.wait()

    def sib_copy(j):
        return pltpu.make_async_remote_copy(
            src_ref=part.at[j, 1 - core],
            dst_ref=from_sib.at[j],
            send_sem=out_send.at[0],
            recv_sem=sib_recv.at[j],
            device_id={"tp": sibling},
            device_id_type=MESH,
        )

    def pair_copy(j, step):
        return pltpu.make_async_remote_copy(
            src_ref=pair_out.at[j, step - 1],
            dst_ref=pair_in.at[j, step - 1],
            send_sem=out_send.at[1],
            recv_sem=pair_recv.at[j, step - 1],
            device_id={"tp": far(step) * 2 + core},
            device_id_type=MESH,
        )

    def out_sent(slots, kind):
        pltpu.make_async_remote_copy(
            src_ref=slots,
            dst_ref=slots,
            send_sem=out_send.at[kind],
            recv_sem=sib_recv.at[0],
            device_id={"tp": sibling},
            device_id_type=MESH,
        ).wait_send()

    for j in range(chunks):
        partial = jnp.dot(
            heads[...], wo[:, j * width : (j + 1) * width], preferred_element_type=F32
        ).astype(BF16)
        for p in range(pairs):
            for c in range(2):
                at = (p * 2 + c) * rows
                part[j, c, p] = partial[at : at + rows]
        sib_copy(j).start()
    for j in range(chunks):
        sib_copy(j).wait_recv()
        for step in range(1, pairs):
            goal = far(step)
            pair_out[j, step - 1] = (
                part[j, core, goal].astype(F32) + from_sib[j, goal].astype(F32)
            ).astype(BF16)
            pair_copy(j, step).start()
    tok_copy(tok.at[:, 0], tok_send.at[0], tok_recv.at[0], sibling).wait_send()
    fwd = tok.at[pl.ds(0, pairs - 1), 0]
    tok_copy(fwd, tok_send.at[1], tok_recv.at[0], sibling).wait_send()

    def drain(d, carried):
        sent(d)
        return carried

    lax.fori_loop(0, outer + 1, drain, 0)
    out_sent(part.at[:, 0], 0)
    for j in range(chunks):
        result = part[j, core, pair].astype(F32) + from_sib[j, pair].astype(F32)
        for step in range(1, pairs):
            pair_copy(j, step).wait_recv()
            result = result + pair_in[j, step - 1].astype(F32)
        out_ref[:, j * width : (j + 1) * width] = result.astype(BF16)

    out_sent(pair_out, 1)


def body(sp_size, tp_size, tokens, w_query, w_key, w_value, w_out, lambda_head, sub_gain):
    rows, depth = tokens.shape
    pairs = tp_size // 2
    count = rows * tp_size
    key_cols = w_key.shape[1]
    groups = key_cols // (2 * QK)
    out_cols = w_out.shape[1]
    chunks = math.gcd(out_cols // 128, 4)
    width = out_cols // chunks
    anywhere = pl.BlockSpec(memory_space=pl.ANY)
    dma = pltpu.SemaphoreType.DMA
    return pl.pallas_call(
        functools.partial(kernel, sp_size, tp_size),
        out_shape=pltpu.VMEM((rows, out_cols), BF16),
        in_specs=[anywhere] * 5
        + [pl.BlockSpec(memory_space=pltpu.SMEM), pl.BlockSpec(memory_space=pltpu.VMEM)],
        out_specs=pl.BlockSpec(memory_space=pltpu.VMEM),
        scratch_shapes=[
            pltpu.VMEM((pairs, 2, 2, rows // 2, depth), BF16),
            pltpu.VMEM(w_query.shape, BF16),
            pltpu.VMEM((2, *w_key.shape), BF16),
            pltpu.VMEM(w_out.shape, BF16),
            pltpu.VMEM((sp_size, pairs, 2, 2, 2, rows // 2, key_cols), BF16),
            pltpu.VMEM((groups, 2 * QK, 4 * count), BF16),
            pltpu.VMEM((groups, VD, 4 * count), F32),
            pltpu.VMEM((groups, 1, 4 * count), F32),
            pltpu.VMEM((groups, 1, 4 * count), F32),
            pltpu.VMEM((count, groups * 2 * VD), BF16),
            pltpu.VMEM((chunks, 2, pairs, rows, width), BF16),
            pltpu.VMEM((chunks, pairs, rows, width), BF16),
            pltpu.VMEM((chunks, pairs - 1, rows, width), BF16),
            pltpu.VMEM((chunks, pairs - 1, rows, width), BF16),
            dma((4,)),
            dma((2,)),
            dma((1 + 4 * (pairs - 1),)),
            dma(((sp_size + 1) // 2,)),
            dma(((sp_size + 1) // 2,)),
            dma((sp_size, 2 + 4 * (pairs - 1))),
            dma((2,)),
            dma((chunks,)),
            dma((chunks, pairs - 1)),
        ],
        compiler_params=pltpu.CompilerParams(
            collective_id=0, has_side_effects=True, vmem_limit_bytes=60 * 1024 * 1024
        ),
    )(tokens, w_query, w_key, w_value, w_out, lambda_head, sub_gain.reshape(1, VD))


def solution(mesh):
    return jax.shard_map(
        functools.partial(body, mesh.shape["sp"], mesh.shape["tp"]),
        mesh=mesh,
        in_specs=(
            P(("sp", "tp"), None),
            P(None, "tp"),
            P(None, "tp"),
            P(None, "tp"),
            P("tp", None),
            P("tp"),
            P(),
        ),
        out_specs=P(("sp", "tp"), None),
        check_vma=False,
    )
```

```python
import functools
import math

import jax
import jax.numpy as jnp
from jax import lax
from jax.experimental import pallas as pl
from jax.experimental.pallas import tpu as pltpu
from jax.sharding import PartitionSpec as P

QK = 64
VD = 128
MESH = pl.DeviceIdType.MESH
F32 = jnp.float32
BF16 = jnp.bfloat16


def kernel(
    sp_size,
    tp_size,
    tok_hbm,
    wq_hbm,
    wk_hbm,
    wv_hbm,
    wo_hbm,
    lam_ref,
    gain_ref,
    out_ref,
    tok,
    wq,
    wkv,
    wo,
    kv,
    q_t,
    acc,
    peak,
    total,
    heads,
    part,
    from_sib,
    pair_out,
    pair_in,
    load_sem,
    tok_send,
    tok_recv,
    kv_next,
    kv_side,
    kv_recv,
    out_send,
    sib_recv,
    pair_recv,
):
    pairs = tp_size // 2
    half = tok.shape[3]
    rows = 2 * half
    depth = tok.shape[4]
    count = pairs * 2 * rows
    key_cols = wkv.shape[2]
    groups = key_cols // (2 * QK)
    chunks, width = part.shape[0], part.shape[4]

    sp = lax.axis_index("sp")
    tp = lax.axis_index("tp")
    pair = tp // 2
    core = lax.rem(tp, 2)
    sibling = tp + 1 - 2 * core
    inner = lax.rem(sp, 2)
    outer = sp // 2
    side = sp + 1 - 2 * inner
    has_next = sp + 2 < sp_size
    has_prev = sp >= 2

    def far(step):
        return lax.rem(pair + step, pairs)

    def near(step):
        return lax.rem(pair + pairs - step, pairs)

    for h in range(2):
        pltpu.make_async_copy(
            tok_hbm.at[pl.ds(h * half, half)], tok.at[pair, core, h], load_sem.at[0]
        ).start()
    load_tok = pltpu.make_async_copy(tok.at[pair, core], tok.at[pair, core], load_sem.at[0])
    pltpu.make_async_copy(wk_hbm, wkv.at[0], load_sem.at[1]).start()
    pltpu.make_async_copy(wv_hbm, wkv.at[1], load_sem.at[1]).start()
    load_kv = pltpu.make_async_copy(wkv, wkv, load_sem.at[1])
    load_wq = pltpu.make_async_copy(wq_hbm, wq, load_sem.at[2])
    load_wo = pltpu.make_async_copy(wo_hbm, wo, load_sem.at[3])
    load_wq.start()
    load_wo.start()

    barrier = pltpu.get_barrier_semaphore()
    pl.semaphore_signal(barrier, inc=1, device_id={"tp": sibling}, device_id_type=MESH)
    for step in range(1, pairs):
        pl.semaphore_signal(
            barrier, inc=1, device_id={"tp": far(step) * 2 + core}, device_id_type=MESH
        )
    pl.semaphore_signal(barrier, inc=1, device_id={"sp": side}, device_id_type=MESH)

    @pl.when(has_next)
    def _():
        pl.semaphore_signal(barrier, inc=1, device_id={"sp": sp + 2}, device_id_type=MESH)

    @pl.when(has_prev)
    def _():
        pl.semaphore_signal(barrier, inc=1, device_id={"sp": sp - 2}, device_id_type=MESH)

    pl.semaphore_wait(barrier, 1 + pairs + has_next.astype(jnp.int32) + has_prev.astype(jnp.int32))

    def tok_copy(slot, sem, recv, device):
        return pltpu.make_async_remote_copy(
            src_ref=slot,
            dst_ref=slot,
            send_sem=sem,
            recv_sem=recv,
            device_id={"tp": device},
            device_id_type=MESH,
        )

    def far_recv(step, role, h):
        return tok_recv.at[1 + ((step - 1) * 2 + role) * 2 + h]

    load_tok.wait()
    for h in range(2):
        for step in range(1, pairs):
            slot = tok.at[pair, core, h]
            goal = far(step) * 2 + core
            tok_copy(slot, tok_send.at[0], far_recv(step, 0, h), goal).start()
        if h == 0:
            tok_copy(tok.at[pair, core], tok_send.at[0], tok_recv.at[0], sibling).start()

    other = 1 - core
    cores = (core, other)

    def kv_at(block, step, role, h):
        chunk = near(step) if step else pair
        if step == 0:
            return kv.at[block, chunk, cores[role]], kv_recv.at[block, role]
        return (
            kv.at[block, chunk, cores[role], h],
            kv_recv.at[block, 2 + ((step - 1) * 2 + role) * 2 + h],
        )

    def kv_copy(slot, sem, recv, device):
        return pltpu.make_async_remote_copy(
            src_ref=slot,
            dst_ref=slot,
            send_sem=sem,
            recv_sem=recv,
            device_id={"sp": device},
            device_id_type=MESH,
        )

    def pass_on(d, step, role, h):
        block = sp - 2 * d
        slot, recv = kv_at(block, step, role, h)

        @pl.when(has_next)
        def _():
            kv_copy(slot, kv_next.at[d], recv, sp + 2).start()

        @pl.when(block < side)
        def _():
            kv_copy(slot, kv_side.at[d], recv, side).start()

    def sent(d):
        whole = kv.at[sp - 2 * d]
        recv = kv_recv.at[0, 0]

        @pl.when(has_next)
        def _():
            kv_copy(whole, kv_next.at[d], recv, sp + 2).wait_send()

        @pl.when(sp - 2 * d < side)
        def _():
            kv_copy(whole, kv_side.at[d], recv, side).wait_send()

    def arrived(block, step, role, h):
        slot, recv = kv_at(block, step, role, h)
        kv_copy(slot, kv_side.at[0], recv, side).wait_recv()

    def relay(d, step, role, h):
        arrived(sp - 2 * d, step, role, h)
        pass_on(d, step, role, h)

    def relay_near(d, role):
        @pl.when(d <= outer)
        def _():
            relay(d, 0, role, 0)

    def relay_far(d, role, h):
        @pl.when(d <= outer)
        def _():
            for step in range(1, pairs):
                relay(d, step, role, h)

    gain_t = jnp.broadcast_to(gain_ref[...], (count, VD)).T
    def project_near(role):
        c = cores[role]
        x = tok[pair, c].reshape(rows, depth)
        for s in range(2):
            made = jnp.dot(x, wkv[s], preferred_element_type=F32).astype(BF16)
            for h in range(2):
                kv[sp, pair, c, h, s] = made[h * half : (h + 1) * half]
        pass_on(0, 0, role, 0)

    def project_far(role, h):
        c = cores[role]
        for step in range(1, pairs):
            source = near(step)
            for s in range(2):
                kv[sp, source, c, h, s] = jnp.dot(
                    tok[source, c, h], wkv[s], preferred_element_type=F32
                ).astype(BF16)
            pass_on(0, step, role, h)

    def receive(role, h):
        for step in range(1, pairs):
            slot = tok.at[near(step), (core, other)[role], h]
            tok_copy(slot, tok_send.at[0], far_recv(step, role, h), sibling).wait_recv()

    def forward(h):
        receive(0, h)
        for step in range(1, pairs):
            slot = tok.at[near(step), core, h]
            tok_copy(slot, tok_send.at[1], far_recv(step, 1, h), sibling).start()

    load_kv.wait()
    project_near(0)
    tok_copy(tok.at[pair, other], tok_send.at[0], tok_recv.at[0], sibling).wait_recv()
    project_near(1)

    map_of = lax.broadcasted_iota(jnp.int32, (2 * QK, count), 0) // QK

    def ask(only):
        for g in only:
            span = slice(g * 4 * QK, (g + 1) * 4 * QK)
            asked = jnp.dot(
                tok[...].reshape(count, depth), wq[:, span], preferred_element_type=F32
            )
            asked = asked.astype(BF16).astype(F32) * (1.0 / math.sqrt(QK))
            for k in range(2):
                turned = asked[:, k * 2 * QK : (k + 1) * 2 * QK].T
                for m in range(2):
                    q_t[g, :, pl.ds((k * 2 + m) * count, count)] = jnp.where(
                        map_of == m, turned, 0.0
                    ).astype(BF16)

    wide = 4 * count

    def absorb(block, first, only=None):
        for g in range(groups) if only is None else only:
            lanes = slice(g * VD, (g + 1) * VD)
            keys = kv[block, :, :, :, 0, :, lanes].reshape(count, 2 * QK)
            values = kv[block, :, :, :, 1, :, lanes].reshape(count, VD)
            scores = jnp.dot(keys, q_t[g], preferred_element_type=F32)
            if first:
                key_at = lax.broadcasted_iota(jnp.int32, (count, wide), 0)
                query_at = lax.rem(lax.broadcasted_iota(jnp.int32, (count, wide), 1), count)
                scores = jnp.where(key_at <= query_at, scores, -jnp.inf)
            top = jnp.max(scores, axis=0, keepdims=True)
            if not first:
                old = peak[g]
                top = jnp.maximum(top, old)
                fade = jnp.exp(old - top)
            expo = jnp.exp(scores - top)
            amount = jnp.sum(expo, axis=0, keepdims=True)
            summed = lax.dot_general(
                values, expo.astype(BF16), (((0,), (0,)), ((), ())), preferred_element_type=F32
            )
            if not first:
                amount = amount + total[g] * fade
                summed = summed + acc[g] * fade
            peak[g] = top
            total[g] = amount
            acc[g] = summed

    relay_near(1, 0)
    forward(0)
    project_far(0, 0)
    relay_near(1, 1)
    receive(1, 0)
    project_far(1, 0)
    forward(1)
    project_far(0, 1)
    relay_near(2, 0)
    receive(1, 1)
    project_far(1, 1)
    relay_near(2, 1)
    relay_far(1, 0, 0)
    relay_far(1, 1, 0)
    load_wq.wait()
    ask(range(groups // 2))
    ask(range(groups // 2, groups))
    absorb(sp, True, range(groups // 2))
    relay_far(1, 0, 1)
    absorb(sp, True, range(groups // 2, groups))
    relay_far(1, 1, 1)

    def turn(d, carried):
        relay_near(d + 2, 0)
        relay_near(d + 2, 1)
        relay_far(d + 1, 0, 0)
        relay_far(d + 1, 1, 0)
        absorb(sp - 2 * d, False, range(groups // 2))
        relay_far(d + 1, 0, 1)
        absorb(sp - 2 * d, False, range(groups // 2, groups))
        relay_far(d + 1, 1, 1)
        return carried

    lax.fori_loop(1, outer + 1, turn, 0)

    def beside(d, carried):
        block = side - 2 * d
        for role in range(2):
            arrived(block, 0, role, 0)
        for step in range(1, pairs):
            for h in range(2):
                for role in range(2):
                    arrived(block, step, role, h)
        absorb(block, False)
        return carried

    lax.fori_loop(1 - inner, outer + 1, beside, 0)

    for g in range(groups):
        for k in range(2):
            left = pl.ds((k * 2) * count, count)
            right = pl.ds((k * 2 + 1) * count, count)
            mixed = acc[g, :, left] / total[g, :, left] - lam_ref[g * 2 + k] * (
                acc[g, :, right] / total[g, :, right]
            )
            power = jnp.mean(mixed * mixed, axis=0, keepdims=True)
            head = mixed * lax.rsqrt(power + 1e-6) * gain_t
            heads[:, (g * 2 + k) * VD : (g * 2 + k + 1) * VD] = head.T.astype(BF16)

    load_wo.wait()

    def sib_copy(j):
        return pltpu.make_async_remote_copy(
            src_ref=part.at[j, 1 - core],
            dst_ref=from_sib.at[j],
            send_sem=out_send.at[0],
            recv_sem=sib_recv.at[j],
            device_id={"tp": sibling},
            device_id_type=MESH,
        )

    def pair_copy(j, step):
        return pltpu.make_async_remote_copy(
            src_ref=pair_out.at[j, step - 1],
            dst_ref=pair_in.at[j, step - 1],
            send_sem=out_send.at[1],
            recv_sem=pair_recv.at[j, step - 1],
            device_id={"tp": far(step) * 2 + core},
            device_id_type=MESH,
        )

    def out_sent(slots, kind):
        pltpu.make_async_remote_copy(
            src_ref=slots,
            dst_ref=slots,
            send_sem=out_send.at[kind],
            recv_sem=sib_recv.at[0],
            device_id={"tp": sibling},
            device_id_type=MESH,
        ).wait_send()

    for j in range(chunks):
        partial = jnp.dot(
            heads[...], wo[:, j * width : (j + 1) * width], preferred_element_type=F32
        ).astype(BF16)
        for p in range(pairs):
            for c in range(2):
                at = (p * 2 + c) * rows
                part[j, c, p] = partial[at : at + rows]
        sib_copy(j).start()
    for j in range(chunks):
        sib_copy(j).wait_recv()
        for step in range(1, pairs):
            goal = far(step)
            pair_out[j, step - 1] = (
                part[j, core, goal].astype(F32) + from_sib[j, goal].astype(F32)
            ).astype(BF16)
            pair_copy(j, step).start()
    tok_copy(tok.at[:, 0], tok_send.at[0], tok_recv.at[0], sibling).wait_send()
    fwd = tok.at[pl.ds(0, pairs - 1), 0]
    tok_copy(fwd, tok_send.at[1], tok_recv.at[0], sibling).wait_send()

    def drain(d, carried):
        sent(d)
        return carried

    lax.fori_loop(0, outer + 1, drain, 0)
    out_sent(part.at[:, 0], 0)
    for j in range(chunks):
        result = part[j, core, pair].astype(F32) + from_sib[j, pair].astype(F32)
        for step in range(1, pairs):
            pair_copy(j, step).wait_recv()
            result = result + pair_in[j, step - 1].astype(F32)
        out_ref[:, j * width : (j + 1) * width] = result.astype(BF16)

    out_sent(pair_out, 1)


def body(sp_size, tp_size, tokens, w_query, w_key, w_value, w_out, lambda_head, sub_gain):
    rows, depth = tokens.shape
    pairs = tp_size // 2
    count = rows * tp_size
    key_cols = w_key.shape[1]
    groups = key_cols // (2 * QK)
    out_cols = w_out.shape[1]
    chunks = math.gcd(out_cols // 128, 2)
    width = out_cols // chunks
    anywhere = pl.BlockSpec(memory_space=pl.ANY)
    dma = pltpu.SemaphoreType.DMA
    return pl.pallas_call(
        functools.partial(kernel, sp_size, tp_size),
        out_shape=pltpu.VMEM((rows, out_cols), BF16),
        in_specs=[anywhere] * 5
        + [pl.BlockSpec(memory_space=pltpu.SMEM), pl.BlockSpec(memory_space=pltpu.VMEM)],
        out_specs=pl.BlockSpec(memory_space=pltpu.VMEM),
        scratch_shapes=[
            pltpu.VMEM((pairs, 2, 2, rows // 2, depth), BF16),
            pltpu.VMEM(w_query.shape, BF16),
            pltpu.VMEM((2, *w_key.shape), BF16),
            pltpu.VMEM(w_out.shape, BF16),
            pltpu.VMEM((sp_size, pairs, 2, 2, 2, rows // 2, key_cols), BF16),
            pltpu.VMEM((groups, 2 * QK, 4 * count), BF16),
            pltpu.VMEM((groups, VD, 4 * count), F32),
            pltpu.VMEM((groups, 1, 4 * count), F32),
            pltpu.VMEM((groups, 1, 4 * count), F32),
            pltpu.VMEM((count, groups * 2 * VD), BF16),
            pltpu.VMEM((chunks, 2, pairs, rows, width), BF16),
            pltpu.VMEM((chunks, pairs, rows, width), BF16),
            pltpu.VMEM((chunks, pairs - 1, rows, width), BF16),
            pltpu.VMEM((chunks, pairs - 1, rows, width), BF16),
            dma((4,)),
            dma((2,)),
            dma((1 + 4 * (pairs - 1),)),
            dma(((sp_size + 1) // 2,)),
            dma(((sp_size + 1) // 2,)),
            dma((sp_size, 2 + 4 * (pairs - 1))),
            dma((2,)),
            dma((chunks,)),
            dma((chunks, pairs - 1)),
        ],
        compiler_params=pltpu.CompilerParams(
            collective_id=0, has_side_effects=True, vmem_limit_bytes=60 * 1024 * 1024
        ),
    )(tokens, w_query, w_key, w_value, w_out, lambda_head, sub_gain.reshape(1, VD))


def solution(mesh):
    return jax.shard_map(
        functools.partial(body, mesh.shape["sp"], mesh.shape["tp"]),
        mesh=mesh,
        in_specs=(
            P(("sp", "tp"), None),
            P(None, "tp"),
            P(None, "tp"),
            P(None, "tp"),
            P("tp", None),
            P("tp"),
            P(),
        ),
        out_specs=P(("sp", "tp"), None),
        check_vma=False,
    )
```

```python
import functools
import math

import jax
import jax.numpy as jnp
from jax import lax
from jax.experimental import pallas as pl
from jax.experimental.pallas import tpu as pltpu
from jax.sharding import PartitionSpec as P

QK = 64
VD = 128
MESH = pl.DeviceIdType.MESH
F32 = jnp.float32
BF16 = jnp.bfloat16
TURN = 2


def kernel(
    sp_size,
    tp_size,
    tok_hbm,
    wq_hbm,
    wk_hbm,
    wv_hbm,
    wo_hbm,
    lam_ref,
    gain_ref,
    out_ref,
    tok,
    wq,
    wkv,
    wo,
    kv,
    q_t,
    acc,
    peak,
    total,
    heads,
    part,
    from_sib,
    pair_out,
    pair_in,
    load_sem,
    tok_send,
    tok_recv,
    kv_next,
    kv_side,
    kv_diag,
    kv_recv,
    ready,
    out_send,
    sib_recv,
    pair_recv,
):
    pairs = tp_size // 2
    half = tok.shape[3]
    rows = 2 * half
    depth = tok.shape[4]
    count = pairs * 2 * rows
    key_cols = wkv.shape[2]
    groups = key_cols // (2 * QK)
    chunks, width = part.shape[0], part.shape[4]

    sp = lax.axis_index("sp")
    tp = lax.axis_index("tp")
    pair = tp // 2
    core = lax.rem(tp, 2)
    sibling = tp + 1 - 2 * core
    inner = lax.rem(sp, 2)
    outer = sp // 2
    side = sp + 1 - 2 * inner
    has_next = sp + 2 < sp_size
    has_prev = sp >= 2

    def far(step):
        return lax.rem(pair + step, pairs)

    def near(step):
        return lax.rem(pair + pairs - step, pairs)

    for h in range(2):
        pltpu.make_async_copy(
            tok_hbm.at[pl.ds(h * half, half)], tok.at[pair, core, h], load_sem.at[0]
        ).start()
    load_tok = pltpu.make_async_copy(tok.at[pair, core], tok.at[pair, core], load_sem.at[0])
    pltpu.make_async_copy(wk_hbm, wkv.at[0], load_sem.at[1]).start()
    pltpu.make_async_copy(wv_hbm, wkv.at[1], load_sem.at[1]).start()
    load_kv = pltpu.make_async_copy(wkv, wkv, load_sem.at[1])
    load_wq = pltpu.make_async_copy(wq_hbm, wq, load_sem.at[2])
    load_wo = pltpu.make_async_copy(wo_hbm, wo, load_sem.at[3])
    load_wq.start()
    load_wo.start()

    barrier = pltpu.get_barrier_semaphore()
    pl.semaphore_signal(barrier, inc=1, device_id={"tp": sibling}, device_id_type=MESH)
    for step in range(1, pairs):
        pl.semaphore_signal(
            barrier, inc=1, device_id={"tp": far(step) * 2 + core}, device_id_type=MESH
        )
    pl.semaphore_signal(barrier, inc=1, device_id={"sp": side}, device_id_type=MESH)

    @pl.when(has_next)
    def _():
        pl.semaphore_signal(barrier, inc=1, device_id={"sp": sp + 2}, device_id_type=MESH)

    @pl.when(has_prev)
    def _():
        pl.semaphore_signal(barrier, inc=1, device_id={"sp": sp - 2}, device_id_type=MESH)

    pl.semaphore_wait(barrier, 1 + pairs + has_next.astype(jnp.int32) + has_prev.astype(jnp.int32))

    def tok_copy(slot, sem, recv, device):
        return pltpu.make_async_remote_copy(
            src_ref=slot,
            dst_ref=slot,
            send_sem=sem,
            recv_sem=recv,
            device_id={"tp": device},
            device_id_type=MESH,
        )

    def far_recv(step, role, h):
        return tok_recv.at[1 + ((step - 1) * 2 + role) * 2 + h]

    load_tok.wait()
    for h in range(2):
        for step in range(1, pairs):
            slot = tok.at[pair, core, h]
            goal = far(step) * 2 + core
            tok_copy(slot, tok_send.at[0], far_recv(step, 0, h), goal).start()
        if h == 0:
            tok_copy(tok.at[pair, core], tok_send.at[0], tok_recv.at[0], sibling).start()

    other = 1 - core
    cores = (core, other)

    @pl.when(has_next)
    def _():
        pl.semaphore_signal(ready.at[0], inc=1, device_id={"sp": side}, device_id_type=MESH)

    def kv_at(block, step, role, h):
        chunk = near(step) if step else pair
        if step == 0:
            return kv.at[block, chunk, cores[role]], kv_recv.at[block, role]
        return (
            kv.at[block, chunk, cores[role], h],
            kv_recv.at[block, 2 + ((step - 1) * 2 + role) * 2 + h],
        )

    def kv_copy(slot, sem, recv, device):
        return pltpu.make_async_remote_copy(
            src_ref=slot,
            dst_ref=slot,
            send_sem=sem,
            recv_sem=recv,
            device_id={"sp": device},
            device_id_type=MESH,
        )

    def pass_on(d, step, role, h):
        block = sp - 2 * d
        slot, recv = kv_at(block, step, role, h)
        beside = block < side

        @pl.when(has_next)
        def _():
            kv_copy(slot, kv_next.at[d], recv, sp + 2).start()

        if step and h:
            beside = jnp.logical_and(beside, d <= TURN)

            @pl.when(jnp.logical_and(has_next, d >= TURN))
            def _():
                kv_copy(slot, kv_diag.at[d], recv, side + 2).start()

        @pl.when(beside)
        def _():
            kv_copy(slot, kv_side.at[d], recv, side).start()

    def sent(d):
        block = sp - 2 * d
        whole = kv.at[block]
        recv = kv_recv.at[0, 0]

        @pl.when(has_next)
        def _():
            kv_copy(whole, kv_next.at[d], recv, sp + 2).wait_send()

        @pl.when(jnp.logical_and(has_next, d >= TURN))
        def _():
            late = kv.at[block, pl.ds(0, pairs - 1), :, 0]
            kv_copy(late, kv_diag.at[d], recv, side + 2).wait_send()

        @pl.when(jnp.logical_and(block < side, d <= TURN))
        def _():
            kv_copy(whole, kv_side.at[d], recv, side).wait_send()

        @pl.when(jnp.logical_and(block < side, d > TURN))
        def _():
            rest = kv.at[pl.ds(0, pairs + 1), 0, :, 0]
            kv_copy(rest, kv_side.at[d], recv, side).wait_send()

    def arrived(block, step, role, h):
        slot, recv = kv_at(block, step, role, h)
        kv_copy(slot, kv_side.at[0], recv, side).wait_recv()

    def relay(d, step, role, h):
        arrived(sp - 2 * d, step, role, h)
        pass_on(d, step, role, h)

    def relay_near(d, role):
        @pl.when(d <= outer)
        def _():
            relay(d, 0, role, 0)

    def relay_far(d, role, h):
        @pl.when(d <= outer)
        def _():
            for step in range(1, pairs):
                relay(d, step, role, h)

    gain_t = jnp.broadcast_to(gain_ref[...], (count, VD)).T
    def project_near(role):
        c = cores[role]
        x = tok[pair, c].reshape(rows, depth)
        for s in range(2):
            made = jnp.dot(x, wkv[s], preferred_element_type=F32).astype(BF16)
            for h in range(2):
                kv[sp, pair, c, h, s] = made[h * half : (h + 1) * half]
        pass_on(0, 0, role, 0)

    def project_far(role, h):
        c = cores[role]
        for step in range(1, pairs):
            source = near(step)
            for s in range(2):
                kv[sp, source, c, h, s] = jnp.dot(
                    tok[source, c, h], wkv[s], preferred_element_type=F32
                ).astype(BF16)
            pass_on(0, step, role, h)

    def receive(role, h):
        for step in range(1, pairs):
            slot = tok.at[near(step), (core, other)[role], h]
            tok_copy(slot, tok_send.at[0], far_recv(step, role, h), sibling).wait_recv()

    def forward(h):
        receive(0, h)
        for step in range(1, pairs):
            slot = tok.at[near(step), core, h]
            tok_copy(slot, tok_send.at[1], far_recv(step, 1, h), sibling).start()

    load_kv.wait()
    project_near(0)
    tok_copy(tok.at[pair, other], tok_send.at[0], tok_recv.at[0], sibling).wait_recv()
    project_near(1)

    map_of = lax.broadcasted_iota(jnp.int32, (2 * QK, count), 0) // QK

    def ask(only):
        for g in only:
            span = slice(g * 4 * QK, (g + 1) * 4 * QK)
            asked = jnp.dot(
                tok[...].reshape(count, depth), wq[:, span], preferred_element_type=F32
            )
            asked = asked.astype(BF16).astype(F32) * (1.0 / math.sqrt(QK))
            for k in range(2):
                turned = asked[:, k * 2 * QK : (k + 1) * 2 * QK].T
                for m in range(2):
                    q_t[g, :, pl.ds((k * 2 + m) * count, count)] = jnp.where(
                        map_of == m, turned, 0.0
                    ).astype(BF16)

    wide = 4 * count

    def absorb(block, first, only=None):
        for g in range(groups) if only is None else only:
            lanes = slice(g * VD, (g + 1) * VD)
            keys = kv[block, :, :, :, 0, :, lanes].reshape(count, 2 * QK)
            values = kv[block, :, :, :, 1, :, lanes].reshape(count, VD)
            scores = jnp.dot(keys, q_t[g], preferred_element_type=F32)
            if first:
                key_at = lax.broadcasted_iota(jnp.int32, (count, wide), 0)
                query_at = lax.rem(lax.broadcasted_iota(jnp.int32, (count, wide), 1), count)
                scores = jnp.where(key_at <= query_at, scores, -jnp.inf)
            top = jnp.max(scores, axis=0, keepdims=True)
            if not first:
                old = peak[g]
                top = jnp.maximum(top, old)
                fade = jnp.exp(old - top)
            expo = jnp.exp(scores - top)
            amount = jnp.sum(expo, axis=0, keepdims=True)
            summed = lax.dot_general(
                values, expo.astype(BF16), (((0,), (0,)), ((), ())), preferred_element_type=F32
            )
            if not first:
                amount = amount + total[g] * fade
                summed = summed + acc[g] * fade
            peak[g] = top
            total[g] = amount
            acc[g] = summed

    relay_near(1, 0)
    forward(0)
    project_far(0, 0)
    relay_near(1, 1)
    receive(1, 0)
    project_far(1, 0)
    forward(1)
    project_far(0, 1)
    @pl.when(has_next)
    def _():
        pl.semaphore_wait(ready.at[0], 1)

    relay_near(2, 0)
    receive(1, 1)
    project_far(1, 1)
    relay_near(2, 1)
    relay_far(1, 0, 0)
    relay_far(1, 1, 0)
    load_wq.wait()
    ask(range(groups // 2))
    ask(range(groups // 2, groups))
    absorb(sp, True, range(groups // 2))
    relay_far(1, 0, 1)
    absorb(sp, True, range(groups // 2, groups))
    relay_far(1, 1, 1)

    def turn(d, carried):
        relay_near(d + 2, 0)
        relay_near(d + 2, 1)
        relay_far(d + 1, 0, 0)
        relay_far(d + 1, 1, 0)
        absorb(sp - 2 * d, False, range(groups // 2))
        relay_far(d + 1, 0, 1)
        absorb(sp - 2 * d, False, range(groups // 2, groups))
        relay_far(d + 1, 1, 1)
        return carried

    lax.fori_loop(1, outer + 1, turn, 0)

    def beside(d, carried):
        block = side - 2 * d
        for role in range(2):
            arrived(block, 0, role, 0)
        for step in range(1, pairs):
            for h in range(2):
                for role in range(2):
                    arrived(block, step, role, h)
        absorb(block, False)
        return carried

    lax.fori_loop(1 - inner, outer + 1, beside, 0)

    for g in range(groups):
        for k in range(2):
            left = pl.ds((k * 2) * count, count)
            right = pl.ds((k * 2 + 1) * count, count)
            mixed = acc[g, :, left] / total[g, :, left] - lam_ref[g * 2 + k] * (
                acc[g, :, right] / total[g, :, right]
            )
            power = jnp.mean(mixed * mixed, axis=0, keepdims=True)
            head = mixed * lax.rsqrt(power + 1e-6) * gain_t
            heads[:, (g * 2 + k) * VD : (g * 2 + k + 1) * VD] = head.T.astype(BF16)

    load_wo.wait()

    def sib_copy(j):
        return pltpu.make_async_remote_copy(
            src_ref=part.at[j, 1 - core],
            dst_ref=from_sib.at[j],
            send_sem=out_send.at[0],
            recv_sem=sib_recv.at[j],
            device_id={"tp": sibling},
            device_id_type=MESH,
        )

    def pair_copy(j, step):
        return pltpu.make_async_remote_copy(
            src_ref=pair_out.at[j, step - 1],
            dst_ref=pair_in.at[j, step - 1],
            send_sem=out_send.at[1],
            recv_sem=pair_recv.at[j, step - 1],
            device_id={"tp": far(step) * 2 + core},
            device_id_type=MESH,
        )

    def out_sent(slots, kind):
        pltpu.make_async_remote_copy(
            src_ref=slots,
            dst_ref=slots,
            send_sem=out_send.at[kind],
            recv_sem=sib_recv.at[0],
            device_id={"tp": sibling},
            device_id_type=MESH,
        ).wait_send()

    for j in range(chunks):
        partial = jnp.dot(
            heads[...], wo[:, j * width : (j + 1) * width], preferred_element_type=F32
        ).astype(BF16)
        for p in range(pairs):
            for c in range(2):
                at = (p * 2 + c) * rows
                part[j, c, p] = partial[at : at + rows]
        sib_copy(j).start()
    for j in range(chunks):
        sib_copy(j).wait_recv()
        for step in range(1, pairs):
            goal = far(step)
            pair_out[j, step - 1] = (
                part[j, core, goal].astype(F32) + from_sib[j, goal].astype(F32)
            ).astype(BF16)
            pair_copy(j, step).start()
    tok_copy(tok.at[:, 0], tok_send.at[0], tok_recv.at[0], sibling).wait_send()
    fwd = tok.at[pl.ds(0, pairs - 1), 0]
    tok_copy(fwd, tok_send.at[1], tok_recv.at[0], sibling).wait_send()

    def drain(d, carried):
        sent(d)
        return carried

    lax.fori_loop(0, outer + 1, drain, 0)
    out_sent(part.at[:, 0], 0)
    for j in range(chunks):
        result = part[j, core, pair].astype(F32) + from_sib[j, pair].astype(F32)
        for step in range(1, pairs):
            pair_copy(j, step).wait_recv()
            result = result + pair_in[j, step - 1].astype(F32)
        out_ref[:, j * width : (j + 1) * width] = result.astype(BF16)

    out_sent(pair_out, 1)


def body(sp_size, tp_size, tokens, w_query, w_key, w_value, w_out, lambda_head, sub_gain):
    rows, depth = tokens.shape
    pairs = tp_size // 2
    count = rows * tp_size
    key_cols = w_key.shape[1]
    groups = key_cols // (2 * QK)
    out_cols = w_out.shape[1]
    chunks = math.gcd(out_cols // 128, 2)
    width = out_cols // chunks
    anywhere = pl.BlockSpec(memory_space=pl.ANY)
    dma = pltpu.SemaphoreType.DMA
    return pl.pallas_call(
        functools.partial(kernel, sp_size, tp_size),
        out_shape=pltpu.VMEM((rows, out_cols), BF16),
        in_specs=[anywhere] * 5
        + [pl.BlockSpec(memory_space=pltpu.SMEM), pl.BlockSpec(memory_space=pltpu.VMEM)],
        out_specs=pl.BlockSpec(memory_space=pltpu.VMEM),
        scratch_shapes=[
            pltpu.VMEM((pairs, 2, 2, rows // 2, depth), BF16),
            pltpu.VMEM(w_query.shape, BF16),
            pltpu.VMEM((2, *w_key.shape), BF16),
            pltpu.VMEM(w_out.shape, BF16),
            pltpu.VMEM((sp_size, pairs, 2, 2, 2, rows // 2, key_cols), BF16),
            pltpu.VMEM((groups, 2 * QK, 4 * count), BF16),
            pltpu.VMEM((groups, VD, 4 * count), F32),
            pltpu.VMEM((groups, 1, 4 * count), F32),
            pltpu.VMEM((groups, 1, 4 * count), F32),
            pltpu.VMEM((count, groups * 2 * VD), BF16),
            pltpu.VMEM((chunks, 2, pairs, rows, width), BF16),
            pltpu.VMEM((chunks, pairs, rows, width), BF16),
            pltpu.VMEM((chunks, pairs - 1, rows, width), BF16),
            pltpu.VMEM((chunks, pairs - 1, rows, width), BF16),
            dma((4,)),
            dma((2,)),
            dma((1 + 4 * (pairs - 1),)),
            dma(((sp_size + 1) // 2,)),
            dma(((sp_size + 1) // 2,)),
            dma(((sp_size + 1) // 2,)),
            dma((sp_size, 2 + 4 * (pairs - 1))),
            pltpu.SemaphoreType.REGULAR((1,)),
            dma((2,)),
            dma((chunks,)),
            dma((chunks, pairs - 1)),
        ],
        compiler_params=pltpu.CompilerParams(
            collective_id=0, has_side_effects=True, vmem_limit_bytes=60 * 1024 * 1024
        ),
    )(tokens, w_query, w_key, w_value, w_out, lambda_head, sub_gain.reshape(1, VD))


def solution(mesh):
    return jax.shard_map(
        functools.partial(body, mesh.shape["sp"], mesh.shape["tp"]),
        mesh=mesh,
        in_specs=(
            P(("sp", "tp"), None),
            P(None, "tp"),
            P(None, "tp"),
            P(None, "tp"),
            P("tp", None),
            P("tp"),
            P(),
        ),
        out_specs=P(("sp", "tp"), None),
        check_vma=False,
    )
```

```python
import functools
import math

import jax
import jax.numpy as jnp
from jax import lax
from jax.experimental import pallas as pl
from jax.experimental.pallas import tpu as pltpu
from jax.sharding import PartitionSpec as P

QK = 64
VD = 128
MESH = pl.DeviceIdType.MESH
F32 = jnp.float32
BF16 = jnp.bfloat16
TURN = 2


def kernel(
    sp_size,
    tp_size,
    tok_hbm,
    wq_hbm,
    wk_hbm,
    wv_hbm,
    wo_hbm,
    lam_ref,
    gain_ref,
    out_ref,
    tok,
    wq,
    wkv,
    wo,
    kv,
    q_t,
    acc,
    peak,
    total,
    heads,
    part,
    from_sib,
    pair_out,
    pair_in,
    load_sem,
    tok_send,
    tok_recv,
    kv_next,
    kv_side,
    kv_diag,
    kv_recv,
    ready,
    out_send,
    sib_recv,
    pair_recv,
):
    pairs = tp_size // 2
    half = tok.shape[3]
    rows = 2 * half
    depth = tok.shape[4]
    count = pairs * 2 * rows
    key_cols = wkv.shape[2]
    groups = key_cols // (2 * QK)
    chunks, width = part.shape[0], part.shape[4]

    sp = lax.axis_index("sp")
    tp = lax.axis_index("tp")
    pair = tp // 2
    core = lax.rem(tp, 2)
    sibling = tp + 1 - 2 * core
    inner = lax.rem(sp, 2)
    outer = sp // 2
    side = sp + 1 - 2 * inner
    has_next = sp + 2 < sp_size
    has_prev = sp >= 2

    def far(step):
        return lax.rem(pair + step, pairs)

    def near(step):
        return lax.rem(pair + pairs - step, pairs)

    for h in range(2):
        pltpu.make_async_copy(
            tok_hbm.at[pl.ds(h * half, half)], tok.at[pair, core, h], load_sem.at[0]
        ).start()
    load_tok = pltpu.make_async_copy(tok.at[pair, core], tok.at[pair, core], load_sem.at[0])
    pltpu.make_async_copy(wk_hbm, wkv.at[0], load_sem.at[1]).start()
    pltpu.make_async_copy(wv_hbm, wkv.at[1], load_sem.at[1]).start()
    load_kv = pltpu.make_async_copy(wkv, wkv, load_sem.at[1])
    load_wq = pltpu.make_async_copy(wq_hbm, wq, load_sem.at[2])
    load_wo = pltpu.make_async_copy(wo_hbm, wo, load_sem.at[3])
    load_wq.start()
    load_wo.start()

    barrier = pltpu.get_barrier_semaphore()
    pl.semaphore_signal(barrier, inc=1, device_id={"tp": sibling}, device_id_type=MESH)
    for step in range(1, pairs):
        pl.semaphore_signal(
            barrier, inc=1, device_id={"tp": far(step) * 2 + core}, device_id_type=MESH
        )
    pl.semaphore_signal(barrier, inc=1, device_id={"sp": side}, device_id_type=MESH)

    @pl.when(has_next)
    def _():
        pl.semaphore_signal(barrier, inc=1, device_id={"sp": sp + 2}, device_id_type=MESH)

    @pl.when(has_prev)
    def _():
        pl.semaphore_signal(barrier, inc=1, device_id={"sp": sp - 2}, device_id_type=MESH)

    pl.semaphore_wait(barrier, 1 + pairs + has_next.astype(jnp.int32) + has_prev.astype(jnp.int32))

    def tok_copy(slot, sem, recv, device):
        return pltpu.make_async_remote_copy(
            src_ref=slot,
            dst_ref=slot,
            send_sem=sem,
            recv_sem=recv,
            device_id={"tp": device},
            device_id_type=MESH,
        )

    def far_recv(step, role, h):
        return tok_recv.at[1 + ((step - 1) * 2 + role) * 2 + h]

    load_tok.wait()
    for h in range(2):
        for step in range(1, pairs):
            slot = tok.at[pair, core, h]
            goal = far(step) * 2 + core
            tok_copy(slot, tok_send.at[0], far_recv(step, 0, h), goal).start()
        if h == 0:
            tok_copy(tok.at[pair, core], tok_send.at[0], tok_recv.at[0], sibling).start()

    other = 1 - core
    cores = (core, other)

    @pl.when(has_next)
    def _():
        pl.semaphore_signal(ready.at[0], inc=1, device_id={"sp": side}, device_id_type=MESH)

    def kv_at(block, step, role, h):
        chunk = near(step) if step else pair
        if step == 0:
            return kv.at[block, chunk, cores[role]], kv_recv.at[block, role]
        return (
            kv.at[block, chunk, cores[role], h],
            kv_recv.at[block, 2 + ((step - 1) * 2 + role) * 2 + h],
        )

    def kv_copy(slot, sem, recv, device):
        return pltpu.make_async_remote_copy(
            src_ref=slot,
            dst_ref=slot,
            send_sem=sem,
            recv_sem=recv,
            device_id={"sp": device},
            device_id_type=MESH,
        )

    def pass_on(d, step, role, h):
        block = sp - 2 * d
        slot, recv = kv_at(block, step, role, h)
        beside = block < side

        @pl.when(has_next)
        def _():
            kv_copy(slot, kv_next.at[d], recv, sp + 2).start()

        if step and h:
            beside = jnp.logical_and(beside, d <= TURN)

            @pl.when(jnp.logical_and(has_next, d >= TURN))
            def _():
                kv_copy(slot, kv_diag.at[d], recv, side + 2).start()

        @pl.when(beside)
        def _():
            kv_copy(slot, kv_side.at[d], recv, side).start()

    def sent(d):
        block = sp - 2 * d
        whole = kv.at[block]
        recv = kv_recv.at[0, 0]

        @pl.when(has_next)
        def _():
            kv_copy(whole, kv_next.at[d], recv, sp + 2).wait_send()

        @pl.when(jnp.logical_and(has_next, d >= TURN))
        def _():
            late = kv.at[block, pl.ds(0, pairs - 1), :, 0]
            kv_copy(late, kv_diag.at[d], recv, side + 2).wait_send()

        @pl.when(jnp.logical_and(block < side, d <= TURN))
        def _():
            kv_copy(whole, kv_side.at[d], recv, side).wait_send()

        @pl.when(jnp.logical_and(block < side, d > TURN))
        def _():
            rest = kv.at[pl.ds(0, pairs + 1), 0, :, 0]
            kv_copy(rest, kv_side.at[d], recv, side).wait_send()

    def arrived(block, step, role, h):
        slot, recv = kv_at(block, step, role, h)
        kv_copy(slot, kv_side.at[0], recv, side).wait_recv()

    def relay(d, step, role, h):
        arrived(sp - 2 * d, step, role, h)
        pass_on(d, step, role, h)

    def relay_near(d, role):
        @pl.when(d <= outer)
        def _():
            relay(d, 0, role, 0)

    def relay_far(d, role, h):
        @pl.when(d <= outer)
        def _():
            for step in range(1, pairs):
                relay(d, step, role, h)

    gain_t = jnp.broadcast_to(gain_ref[...], (count, VD)).T
    def project_near(role):
        c = cores[role]
        x = tok[pair, c].reshape(rows, depth)
        for s in range(2):
            made = jnp.dot(x, wkv[s], preferred_element_type=F32).astype(BF16)
            for h in range(2):
                kv[sp, pair, c, h, s] = made[h * half : (h + 1) * half]
        pass_on(0, 0, role, 0)

    def project_far(role, h):
        c = cores[role]
        for step in range(1, pairs):
            source = near(step)
            for s in range(2):
                kv[sp, source, c, h, s] = jnp.dot(
                    tok[source, c, h], wkv[s], preferred_element_type=F32
                ).astype(BF16)
            pass_on(0, step, role, h)

    def receive(role, h):
        for step in range(1, pairs):
            slot = tok.at[near(step), (core, other)[role], h]
            tok_copy(slot, tok_send.at[0], far_recv(step, role, h), sibling).wait_recv()

    def forward(h):
        receive(0, h)
        for step in range(1, pairs):
            slot = tok.at[near(step), core, h]
            tok_copy(slot, tok_send.at[1], far_recv(step, 1, h), sibling).start()

    load_kv.wait()
    project_near(0)
    tok_copy(tok.at[pair, other], tok_send.at[0], tok_recv.at[0], sibling).wait_recv()
    project_near(1)

    map_of = lax.broadcasted_iota(jnp.int32, (2 * QK, count), 0) // QK

    def ask(only):
        for g in only:
            span = slice(g * 4 * QK, (g + 1) * 4 * QK)
            asked = jnp.dot(
                tok[...].reshape(count, depth), wq[:, span], preferred_element_type=F32
            )
            asked = asked.astype(BF16).astype(F32) * (1.0 / math.sqrt(QK))
            for k in range(2):
                turned = asked[:, k * 2 * QK : (k + 1) * 2 * QK].T
                for m in range(2):
                    q_t[g, :, pl.ds((k * 2 + m) * count, count)] = jnp.where(
                        map_of == m, turned, 0.0
                    ).astype(BF16)

    wide = 4 * count

    def absorb(block, first, only=None):
        for g in range(groups) if only is None else only:
            lanes = slice(g * VD, (g + 1) * VD)
            keys = kv[block, :, :, :, 0, :, lanes].reshape(count, 2 * QK)
            values = kv[block, :, :, :, 1, :, lanes].reshape(count, VD)
            scores = jnp.dot(keys, q_t[g], preferred_element_type=F32)
            if first:
                key_at = lax.broadcasted_iota(jnp.int32, (count, wide), 0)
                query_at = lax.rem(lax.broadcasted_iota(jnp.int32, (count, wide), 1), count)
                scores = jnp.where(key_at <= query_at, scores, -jnp.inf)
            top = jnp.max(scores, axis=0, keepdims=True)
            if not first:
                old = peak[g]
                top = jnp.maximum(top, old)
                fade = jnp.exp(old - top)
            expo = jnp.exp(scores - top)
            amount = jnp.sum(expo, axis=0, keepdims=True)
            summed = lax.dot_general(
                values, expo.astype(BF16), (((0,), (0,)), ((), ())), preferred_element_type=F32
            )
            if not first:
                amount = amount + total[g] * fade
                summed = summed + acc[g] * fade
            peak[g] = top
            total[g] = amount
            acc[g] = summed

    relay_near(1, 0)
    forward(0)
    project_far(0, 0)
    relay_near(1, 1)
    receive(1, 0)
    project_far(1, 0)
    forward(1)
    project_far(0, 1)
    @pl.when(has_next)
    def _():
        pl.semaphore_wait(ready.at[0], 1)

    relay_near(2, 0)
    receive(1, 1)
    project_far(1, 1)
    relay_near(2, 1)
    relay_far(1, 0, 0)
    relay_far(1, 1, 0)
    load_wq.wait()
    ask(range(groups // 2))
    ask(range(groups // 2, groups))
    absorb(sp, True, range(groups // 2))
    relay_far(1, 0, 1)
    absorb(sp, True, range(groups // 2, groups))
    relay_far(1, 1, 1)

    def take_side(d):
        block = side - 2 * d
        for role in range(2):
            arrived(block, 0, role, 0)
        for step in range(1, pairs):
            for h in range(2):
                for role in range(2):
                    arrived(block, step, role, h)
        absorb(block, False)

    def turn(d, carried):
        relay_near(d + 2, 0)
        relay_near(d + 2, 1)
        relay_far(d + 1, 0, 0)
        relay_far(d + 1, 1, 0)
        absorb(sp - 2 * d, False, range(groups // 2))
        relay_far(d + 1, 0, 1)
        absorb(sp - 2 * d, False, range(groups // 2, groups))
        relay_far(d + 1, 1, 1)

        @pl.when(d - 1 >= 1 - inner)
        def _():
            take_side(d - 1)

        return carried

    lax.fori_loop(1, outer + 1, turn, 0)

    def beside(d, carried):
        take_side(d)
        return carried

    lax.fori_loop(jnp.maximum(1 - inner, outer - 0), outer + 1, beside, 0)

    for g in range(groups):
        for k in range(2):
            left = pl.ds((k * 2) * count, count)
            right = pl.ds((k * 2 + 1) * count, count)
            mixed = acc[g, :, left] * (1.0 / total[g, :, left]) - acc[g, :, right] * (
                lam_ref[g * 2 + k] / total[g, :, right]
            )
            power = jnp.mean(mixed * mixed, axis=0, keepdims=True)
            head = mixed * lax.rsqrt(power + 1e-6) * gain_t
            heads[:, (g * 2 + k) * VD : (g * 2 + k + 1) * VD] = head.astype(BF16).T

    load_wo.wait()

    def sib_copy(j):
        return pltpu.make_async_remote_copy(
            src_ref=part.at[j, 1 - core],
            dst_ref=from_sib.at[j],
            send_sem=out_send.at[0],
            recv_sem=sib_recv.at[j],
            device_id={"tp": sibling},
            device_id_type=MESH,
        )

    def pair_copy(j, step):
        return pltpu.make_async_remote_copy(
            src_ref=pair_out.at[j, step - 1],
            dst_ref=pair_in.at[j, step - 1],
            send_sem=out_send.at[1],
            recv_sem=pair_recv.at[j, step - 1],
            device_id={"tp": far(step) * 2 + core},
            device_id_type=MESH,
        )

    def out_sent(slots, kind):
        pltpu.make_async_remote_copy(
            src_ref=slots,
            dst_ref=slots,
            send_sem=out_send.at[kind],
            recv_sem=sib_recv.at[0],
            device_id={"tp": sibling},
            device_id_type=MESH,
        ).wait_send()

    for j in range(chunks):
        partial = jnp.dot(
            heads[...], wo[:, j * width : (j + 1) * width], preferred_element_type=F32
        ).astype(BF16)
        for p in range(pairs):
            for c in range(2):
                at = (p * 2 + c) * rows
                part[j, c, p] = partial[at : at + rows]
        sib_copy(j).start()
    for j in range(chunks):
        sib_copy(j).wait_recv()
        for step in range(1, pairs):
            goal = far(step)
            pair_out[j, step - 1] = (
                part[j, core, goal].astype(F32) + from_sib[j, goal].astype(F32)
            ).astype(BF16)
            pair_copy(j, step).start()
    tok_copy(tok.at[:, 0], tok_send.at[0], tok_recv.at[0], sibling).wait_send()
    fwd = tok.at[pl.ds(0, pairs - 1), 0]
    tok_copy(fwd, tok_send.at[1], tok_recv.at[0], sibling).wait_send()

    def drain(d, carried):
        sent(d)
        return carried

    lax.fori_loop(0, outer + 1, drain, 0)
    out_sent(part.at[:, 0], 0)
    for j in range(chunks):
        result = part[j, core, pair].astype(F32) + from_sib[j, pair].astype(F32)
        for step in range(1, pairs):
            pair_copy(j, step).wait_recv()
            result = result + pair_in[j, step - 1].astype(F32)
        out_ref[:, j * width : (j + 1) * width] = result.astype(BF16)

    out_sent(pair_out, 1)


def body(sp_size, tp_size, tokens, w_query, w_key, w_value, w_out, lambda_head, sub_gain):
    rows, depth = tokens.shape
    pairs = tp_size // 2
    count = rows * tp_size
    key_cols = w_key.shape[1]
    groups = key_cols // (2 * QK)
    out_cols = w_out.shape[1]
    chunks = math.gcd(out_cols // 128, 2)
    width = out_cols // chunks
    anywhere = pl.BlockSpec(memory_space=pl.ANY)
    dma = pltpu.SemaphoreType.DMA
    return pl.pallas_call(
        functools.partial(kernel, sp_size, tp_size),
        out_shape=pltpu.VMEM((rows, out_cols), BF16),
        in_specs=[anywhere] * 5
        + [pl.BlockSpec(memory_space=pltpu.SMEM), pl.BlockSpec(memory_space=pltpu.VMEM)],
        out_specs=pl.BlockSpec(memory_space=pltpu.VMEM),
        scratch_shapes=[
            pltpu.VMEM((pairs, 2, 2, rows // 2, depth), BF16),
            pltpu.VMEM(w_query.shape, BF16),
            pltpu.VMEM((2, *w_key.shape), BF16),
            pltpu.VMEM(w_out.shape, BF16),
            pltpu.VMEM((sp_size, pairs, 2, 2, 2, rows // 2, key_cols), BF16),
            pltpu.VMEM((groups, 2 * QK, 4 * count), BF16),
            pltpu.VMEM((groups, VD, 4 * count), F32),
            pltpu.VMEM((groups, 1, 4 * count), F32),
            pltpu.VMEM((groups, 1, 4 * count), F32),
            pltpu.VMEM((count, groups * 2 * VD), BF16),
            pltpu.VMEM((chunks, 2, pairs, rows, width), BF16),
            pltpu.VMEM((chunks, pairs, rows, width), BF16),
            pltpu.VMEM((chunks, pairs - 1, rows, width), BF16),
            pltpu.VMEM((chunks, pairs - 1, rows, width), BF16),
            dma((4,)),
            dma((2,)),
            dma((1 + 4 * (pairs - 1),)),
            dma(((sp_size + 1) // 2,)),
            dma(((sp_size + 1) // 2,)),
            dma(((sp_size + 1) // 2,)),
            dma((sp_size, 2 + 4 * (pairs - 1))),
            pltpu.SemaphoreType.REGULAR((1,)),
            dma((2,)),
            dma((chunks,)),
            dma((chunks, pairs - 1)),
        ],
        compiler_params=pltpu.CompilerParams(
            collective_id=0, has_side_effects=True, vmem_limit_bytes=60 * 1024 * 1024
        ),
    )(tokens, w_query, w_key, w_value, w_out, lambda_head, sub_gain.reshape(1, VD))


def solution(mesh):
    return jax.shard_map(
        functools.partial(body, mesh.shape["sp"], mesh.shape["tp"]),
        mesh=mesh,
        in_specs=(
            P(("sp", "tp"), None),
            P(None, "tp"),
            P(None, "tp"),
            P(None, "tp"),
            P("tp", None),
            P("tp"),
            P(),
        ),
        out_specs=P(("sp", "tp"), None),
        check_vma=False,
    )
```

```python
import functools
import math

import jax
import jax.numpy as jnp
from jax import lax
from jax.experimental import pallas as pl
from jax.experimental.pallas import tpu as pltpu
from jax.sharding import PartitionSpec as P

QK = 64
VD = 128
MESH = pl.DeviceIdType.MESH
F32 = jnp.float32
BF16 = jnp.bfloat16
TURN = 2


def kernel(
    sp_size,
    tp_size,
    tok_hbm,
    wq_hbm,
    wk_hbm,
    wv_hbm,
    wo_hbm,
    lam_ref,
    gain_ref,
    out_ref,
    tok,
    wq,
    wkv,
    wo,
    kv,
    q_t,
    acc,
    peak,
    total,
    heads,
    part,
    from_sib,
    pair_out,
    pair_in,
    load_sem,
    tok_send,
    tok_recv,
    kv_next,
    kv_side,
    kv_diag,
    kv_recv,
    ready,
    out_send,
    sib_recv,
    pair_recv,
):
    pairs = tp_size // 2
    half = tok.shape[3]
    rows = 2 * half
    depth = tok.shape[4]
    count = pairs * 2 * rows
    key_cols = wkv.shape[2]
    groups = key_cols // (2 * QK)
    chunks, width = part.shape[0], part.shape[4]

    sp = lax.axis_index("sp")
    tp = lax.axis_index("tp")
    pair = tp // 2
    core = lax.rem(tp, 2)
    sibling = tp + 1 - 2 * core
    inner = lax.rem(sp, 2)
    outer = sp // 2
    side = sp + 1 - 2 * inner
    has_next = sp + 2 < sp_size
    has_prev = sp >= 2

    def far(step):
        return lax.rem(pair + step, pairs)

    def near(step):
        return lax.rem(pair + pairs - step, pairs)

    for h in range(2):
        pltpu.make_async_copy(
            tok_hbm.at[pl.ds(h * half, half)], tok.at[pair, core, h], load_sem.at[0]
        ).start()
    load_tok = pltpu.make_async_copy(tok.at[pair, core], tok.at[pair, core], load_sem.at[0])
    pltpu.make_async_copy(wk_hbm, wkv.at[0], load_sem.at[1]).start()
    pltpu.make_async_copy(wv_hbm, wkv.at[1], load_sem.at[1]).start()
    load_kv = pltpu.make_async_copy(wkv, wkv, load_sem.at[1])
    load_wq = pltpu.make_async_copy(wq_hbm, wq, load_sem.at[2])
    load_wo = pltpu.make_async_copy(wo_hbm, wo, load_sem.at[3])

    barrier = pltpu.get_barrier_semaphore()
    pl.semaphore_signal(barrier, inc=1, device_id={"tp": sibling}, device_id_type=MESH)
    for step in range(1, pairs):
        pl.semaphore_signal(
            barrier, inc=1, device_id={"tp": far(step) * 2 + core}, device_id_type=MESH
        )
    pl.semaphore_signal(barrier, inc=1, device_id={"sp": side}, device_id_type=MESH)

    @pl.when(has_next)
    def _():
        pl.semaphore_signal(barrier, inc=1, device_id={"sp": sp + 2}, device_id_type=MESH)

    @pl.when(has_prev)
    def _():
        pl.semaphore_signal(barrier, inc=1, device_id={"sp": sp - 2}, device_id_type=MESH)

    pl.semaphore_wait(barrier, 1 + pairs + has_next.astype(jnp.int32) + has_prev.astype(jnp.int32))

    def tok_copy(slot, sem, recv, device):
        return pltpu.make_async_remote_copy(
            src_ref=slot,
            dst_ref=slot,
            send_sem=sem,
            recv_sem=recv,
            device_id={"tp": device},
            device_id_type=MESH,
        )

    def far_recv(step, role, h):
        return tok_recv.at[1 + ((step - 1) * 2 + role) * 2 + h]

    load_tok.wait()
    for h in range(2):
        for step in range(1, pairs):
            slot = tok.at[pair, core, h]
            goal = far(step) * 2 + core
            tok_copy(slot, tok_send.at[0], far_recv(step, 0, h), goal).start()
        if h == 0:
            tok_copy(tok.at[pair, core], tok_send.at[0], tok_recv.at[0], sibling).start()

    other = 1 - core
    cores = (core, other)

    @pl.when(has_next)
    def _():
        pl.semaphore_signal(ready.at[0], inc=1, device_id={"sp": side}, device_id_type=MESH)

    def kv_at(block, step, role, h):
        chunk = near(step) if step else pair
        if step == 0:
            return kv.at[block, chunk, cores[role]], kv_recv.at[block, role]
        return (
            kv.at[block, chunk, cores[role], h],
            kv_recv.at[block, 2 + ((step - 1) * 2 + role) * 2 + h],
        )

    def kv_copy(slot, sem, recv, device):
        return pltpu.make_async_remote_copy(
            src_ref=slot,
            dst_ref=slot,
            send_sem=sem,
            recv_sem=recv,
            device_id={"sp": device},
            device_id_type=MESH,
        )

    def pass_on(d, step, role, h):
        block = sp - 2 * d
        slot, recv = kv_at(block, step, role, h)
        beside = block < side

        @pl.when(has_next)
        def _():
            kv_copy(slot, kv_next.at[d], recv, sp + 2).start()

        if step and h:
            beside = jnp.logical_and(beside, d <= TURN)

            @pl.when(jnp.logical_and(has_next, d >= TURN))
            def _():
                kv_copy(slot, kv_diag.at[d], recv, side + 2).start()

        @pl.when(beside)
        def _():
            kv_copy(slot, kv_side.at[d], recv, side).start()

    def sent(d):
        block = sp - 2 * d
        whole = kv.at[block]
        recv = kv_recv.at[0, 0]

        @pl.when(has_next)
        def _():
            kv_copy(whole, kv_next.at[d], recv, sp + 2).wait_send()

        @pl.when(jnp.logical_and(has_next, d >= TURN))
        def _():
            late = kv.at[block, pl.ds(0, pairs - 1), :, 0]
            kv_copy(late, kv_diag.at[d], recv, side + 2).wait_send()

        @pl.when(jnp.logical_and(block < side, d <= TURN))
        def _():
            kv_copy(whole, kv_side.at[d], recv, side).wait_send()

        @pl.when(jnp.logical_and(block < side, d > TURN))
        def _():
            rest = kv.at[pl.ds(0, pairs + 1), 0, :, 0]
            kv_copy(rest, kv_side.at[d], recv, side).wait_send()

    def arrived(block, step, role, h):
        slot, recv = kv_at(block, step, role, h)
        kv_copy(slot, kv_side.at[0], recv, side).wait_recv()

    def relay(d, step, role, h):
        arrived(sp - 2 * d, step, role, h)
        pass_on(d, step, role, h)

    def relay_near(d, role):
        @pl.when(d <= outer)
        def _():
            relay(d, 0, role, 0)

    def relay_far(d, role, h):
        @pl.when(d <= outer)
        def _():
            for step in range(1, pairs):
                relay(d, step, role, h)

    gain_t = jnp.broadcast_to(gain_ref[...], (count, VD)).T
    def project_near(role):
        c = cores[role]
        x = tok[pair, c].reshape(rows, depth)
        for s in range(2):
            made = jnp.dot(x, wkv[s], preferred_element_type=F32).astype(BF16)
            for h in range(2):
                kv[sp, pair, c, h, s] = made[h * half : (h + 1) * half]
        pass_on(0, 0, role, 0)

    def project_far(role, h):
        c = cores[role]
        for step in range(1, pairs):
            source = near(step)
            for s in range(2):
                kv[sp, source, c, h, s] = jnp.dot(
                    tok[source, c, h], wkv[s], preferred_element_type=F32
                ).astype(BF16)
            pass_on(0, step, role, h)

    def receive(role, h):
        for step in range(1, pairs):
            slot = tok.at[near(step), (core, other)[role], h]
            tok_copy(slot, tok_send.at[0], far_recv(step, role, h), sibling).wait_recv()

    def forward(h):
        receive(0, h)
        for step in range(1, pairs):
            slot = tok.at[near(step), core, h]
            tok_copy(slot, tok_send.at[1], far_recv(step, 1, h), sibling).start()

    load_kv.wait()
    load_wq.start()
    load_wo.start()
    project_near(0)
    tok_copy(tok.at[pair, other], tok_send.at[0], tok_recv.at[0], sibling).wait_recv()
    project_near(1)

    map_of = lax.broadcasted_iota(jnp.int32, (2 * QK, count), 0) // QK

    def ask(only):
        for g in only:
            span = slice(g * 4 * QK, (g + 1) * 4 * QK)
            asked = jnp.dot(
                tok[...].reshape(count, depth), wq[:, span], preferred_element_type=F32
            )
            asked = asked.astype(BF16).astype(F32) * (1.0 / math.sqrt(QK))
            for k in range(2):
                turned = asked[:, k * 2 * QK : (k + 1) * 2 * QK].T
                for m in range(2):
                    q_t[g, :, pl.ds((k * 2 + m) * count, count)] = jnp.where(
                        map_of == m, turned, 0.0
                    ).astype(BF16)

    wide = 4 * count

    def absorb(block, first, only=None):
        for g in range(groups) if only is None else only:
            lanes = slice(g * VD, (g + 1) * VD)
            keys = kv[block, :, :, :, 0, :, lanes].reshape(count, 2 * QK)
            values = kv[block, :, :, :, 1, :, lanes].reshape(count, VD)
            scores = jnp.dot(keys, q_t[g], preferred_element_type=F32)
            if first:
                key_at = lax.broadcasted_iota(jnp.int32, (count, wide), 0)
                query_at = lax.rem(lax.broadcasted_iota(jnp.int32, (count, wide), 1), count)
                scores = jnp.where(key_at <= query_at, scores, -jnp.inf)
            top = jnp.max(scores, axis=0, keepdims=True)
            if not first:
                old = peak[g]
                top = jnp.maximum(top, old)
                fade = jnp.exp(old - top)
            expo = jnp.exp(scores - top)
            amount = jnp.sum(expo, axis=0, keepdims=True)
            summed = lax.dot_general(
                values, expo.astype(BF16), (((0,), (0,)), ((), ())), preferred_element_type=F32
            )
            if not first:
                amount = amount + total[g] * fade
                summed = summed + acc[g] * fade
            peak[g] = top
            total[g] = amount
            acc[g] = summed

    relay_near(1, 0)
    forward(0)
    project_far(0, 0)
    relay_near(1, 1)
    receive(1, 0)
    project_far(1, 0)
    forward(1)
    project_far(0, 1)
    @pl.when(has_next)
    def _():
        pl.semaphore_wait(ready.at[0], 1)

    relay_near(2, 0)
    receive(1, 1)
    project_far(1, 1)
    relay_near(2, 1)
    relay_far(1, 0, 0)
    relay_far(1, 1, 0)
    load_wq.wait()
    ask(range(groups // 2))
    ask(range(groups // 2, groups))
    absorb(sp, True, range(groups // 2))
    relay_far(1, 0, 1)
    absorb(sp, True, range(groups // 2, groups))
    relay_far(1, 1, 1)

    def take_side(d):
        block = side - 2 * d
        for role in range(2):
            arrived(block, 0, role, 0)
        for step in range(1, pairs):
            for h in range(2):
                for role in range(2):
                    arrived(block, step, role, h)
        absorb(block, False)

    def turn(d, carried):
        relay_near(d + 2, 0)
        relay_near(d + 2, 1)
        relay_far(d + 1, 0, 0)
        relay_far(d + 1, 1, 0)
        absorb(sp - 2 * d, False, range(groups // 2))
        relay_far(d + 1, 0, 1)
        absorb(sp - 2 * d, False, range(groups // 2, groups))
        relay_far(d + 1, 1, 1)

        @pl.when(d - 1 >= 1 - inner)
        def _():
            take_side(d - 1)

        return carried

    lax.fori_loop(1, outer + 1, turn, 0)

    def beside(d, carried):
        take_side(d)
        return carried

    lax.fori_loop(jnp.maximum(1 - inner, outer - 0), outer + 1, beside, 0)

    for g in range(groups):
        for k in range(2):
            left = pl.ds((k * 2) * count, count)
            right = pl.ds((k * 2 + 1) * count, count)
            mixed = acc[g, :, left] * (1.0 / total[g, :, left]) - acc[g, :, right] * (
                lam_ref[g * 2 + k] / total[g, :, right]
            )
            power = jnp.mean(mixed * mixed, axis=0, keepdims=True)
            head = mixed * lax.rsqrt(power + 1e-6) * gain_t
            heads[:, (g * 2 + k) * VD : (g * 2 + k + 1) * VD] = head.astype(BF16).T

    load_wo.wait()

    def sib_copy(j):
        return pltpu.make_async_remote_copy(
            src_ref=part.at[j, 1 - core],
            dst_ref=from_sib.at[j],
            send_sem=out_send.at[0],
            recv_sem=sib_recv.at[j],
            device_id={"tp": sibling},
            device_id_type=MESH,
        )

    def pair_copy(j, step):
        return pltpu.make_async_remote_copy(
            src_ref=pair_out.at[j, step - 1],
            dst_ref=pair_in.at[j, step - 1],
            send_sem=out_send.at[1],
            recv_sem=pair_recv.at[j, step - 1],
            device_id={"tp": far(step) * 2 + core},
            device_id_type=MESH,
        )

    def out_sent(slots, kind):
        pltpu.make_async_remote_copy(
            src_ref=slots,
            dst_ref=slots,
            send_sem=out_send.at[kind],
            recv_sem=sib_recv.at[0],
            device_id={"tp": sibling},
            device_id_type=MESH,
        ).wait_send()

    for j in range(chunks):
        partial = jnp.dot(
            heads[...], wo[:, j * width : (j + 1) * width], preferred_element_type=F32
        ).astype(BF16)
        for p in range(pairs):
            for c in range(2):
                at = (p * 2 + c) * rows
                part[j, c, p] = partial[at : at + rows]
        sib_copy(j).start()
    for j in range(chunks):
        sib_copy(j).wait_recv()
        for step in range(1, pairs):
            goal = far(step)
            pair_out[j, step - 1] = (
                part[j, core, goal].astype(F32) + from_sib[j, goal].astype(F32)
            ).astype(BF16)
            pair_copy(j, step).start()
    tok_copy(tok.at[:, 0], tok_send.at[0], tok_recv.at[0], sibling).wait_send()
    fwd = tok.at[pl.ds(0, pairs - 1), 0]
    tok_copy(fwd, tok_send.at[1], tok_recv.at[0], sibling).wait_send()

    def drain(d, carried):
        sent(d)
        return carried

    lax.fori_loop(0, outer + 1, drain, 0)
    out_sent(part.at[:, 0], 0)
    for j in range(chunks):
        result = part[j, core, pair].astype(F32) + from_sib[j, pair].astype(F32)
        for step in range(1, pairs):
            pair_copy(j, step).wait_recv()
            result = result + pair_in[j, step - 1].astype(F32)
        out_ref[:, j * width : (j + 1) * width] = result.astype(BF16)

    out_sent(pair_out, 1)


def body(sp_size, tp_size, tokens, w_query, w_key, w_value, w_out, lambda_head, sub_gain):
    rows, depth = tokens.shape
    pairs = tp_size // 2
    count = rows * tp_size
    key_cols = w_key.shape[1]
    groups = key_cols // (2 * QK)
    out_cols = w_out.shape[1]
    chunks = math.gcd(out_cols // 128, 2)
    width = out_cols // chunks
    anywhere = pl.BlockSpec(memory_space=pl.ANY)
    dma = pltpu.SemaphoreType.DMA
    return pl.pallas_call(
        functools.partial(kernel, sp_size, tp_size),
        out_shape=pltpu.VMEM((rows, out_cols), BF16),
        in_specs=[anywhere] * 5
        + [pl.BlockSpec(memory_space=pltpu.SMEM), pl.BlockSpec(memory_space=pltpu.VMEM)],
        out_specs=pl.BlockSpec(memory_space=pltpu.VMEM),
        scratch_shapes=[
            pltpu.VMEM((pairs, 2, 2, rows // 2, depth), BF16),
            pltpu.VMEM(w_query.shape, BF16),
            pltpu.VMEM((2, *w_key.shape), BF16),
            pltpu.VMEM(w_out.shape, BF16),
            pltpu.VMEM((sp_size, pairs, 2, 2, 2, rows // 2, key_cols), BF16),
            pltpu.VMEM((groups, 2 * QK, 4 * count), BF16),
            pltpu.VMEM((groups, VD, 4 * count), F32),
            pltpu.VMEM((groups, 1, 4 * count), F32),
            pltpu.VMEM((groups, 1, 4 * count), F32),
            pltpu.VMEM((count, groups * 2 * VD), BF16),
            pltpu.VMEM((chunks, 2, pairs, rows, width), BF16),
            pltpu.VMEM((chunks, pairs, rows, width), BF16),
            pltpu.VMEM((chunks, pairs - 1, rows, width), BF16),
            pltpu.VMEM((chunks, pairs - 1, rows, width), BF16),
            dma((4,)),
            dma((2,)),
            dma((1 + 4 * (pairs - 1),)),
            dma(((sp_size + 1) // 2,)),
            dma(((sp_size + 1) // 2,)),
            dma(((sp_size + 1) // 2,)),
            dma((sp_size, 2 + 4 * (pairs - 1))),
            pltpu.SemaphoreType.REGULAR((1,)),
            dma((2,)),
            dma((chunks,)),
            dma((chunks, pairs - 1)),
        ],
        compiler_params=pltpu.CompilerParams(
            collective_id=0, has_side_effects=True, vmem_limit_bytes=60 * 1024 * 1024
        ),
    )(tokens, w_query, w_key, w_value, w_out, lambda_head, sub_gain.reshape(1, VD))


def solution(mesh):
    return jax.shard_map(
        functools.partial(body, mesh.shape["sp"], mesh.shape["tp"]),
        mesh=mesh,
        in_specs=(
            P(("sp", "tp"), None),
            P(None, "tp"),
            P(None, "tp"),
            P(None, "tp"),
            P("tp", None),
            P("tp"),
            P(),
        ),
        out_specs=P(("sp", "tp"), None),
        check_vma=False,
    )
```
